128 devices in a mesh: ep: 32 (over z, y, core), tp: 4 (over x).
Axes of the slice: x: 4, y: 4, z: 4, core: 2. Of those that a mesh axis runs over, the one named last changes fastest.
Arguments:
- tokens_first: bfloat16 [16384, 2048], P('ep'), may hold values from -6 to 6
- norm_gain_first: float32 [2048], replicated, may hold values from 0.1 to 1.9
- w_query: bfloat16 [2048, 512], P(None, 'tp'), may hold values from -0.125 to 0.125
- w_key: bfloat16 [2048, 512], P(None, 'tp'), may hold values from -0.125 to 0.125
- w_value: bfloat16 [2048, 1024], P(None, 'tp'), may hold values from -0.125 to 0.125
- w_outgate: bfloat16 [2048, 1024], P(None, 'tp'), may hold values from -0.125 to 0.125
- w_decay: bfloat16 [2048, 512], P(None, 'tp'), may hold values from -1 to 1
- decay_bias: float32 [256, 512], P('ep', 'tp'), may hold values from -1.3 to 12.5
- head_gain: float32 [1024], P('tp'), may hold values from 0.1 to 1.9
- w_mix_out: bfloat16 [1024, 2048], P('tp'), may hold values from -0.1875 to 0.1875
- tokens_second: bfloat16 [8192, 2048], P('ep'), may hold values from -6 to 6
- norm_gain_second: float32 [2048], replicated, may hold values from 0.1 to 1.9
- routes: int32 [8192, 2], P('ep'), may hold values from 0 to 31, all different within a row; in each aligned block of 256 rows (0 to 255, 256 to 511, ...) at most 32 rows name the same one
- route_logits: float32 [8192, 2], P('ep'), may hold values from -8 to 8
- expert_gate: bfloat16 [32, 2048, 3072], P('ep', None, 'tp'), may hold values from -0.125 to 0.125
- expert_up: bfloat16 [32, 2048, 3072], P('ep', None, 'tp'), may hold values from -0.125 to 0.125
- expert_down: bfloat16 [32, 3072, 2048], P('ep', 'tp'), may hold values from -0.109375 to 0.109375
Outputs:
- mixed_first: bfloat16 [16384, 2048], P(('ep', 'tp'))
- mixed_second: bfloat16 [8192, 2048], P('ep', 'tp')
The draws below stay inside these ranges and needn't reach their ends.
Inputs may be any that keep to these rules, and one draw needn't show every extreme that they name: In the rows of one index of ep (aligned blocks of 256 rows) no expert is named by more than 32 rows, a bound that some block reaches; the two routes of a row name different experts.
All inputs are finite; a program needn't handle non-finite values.
Results may differ from the reference program's by a relative error of at most 0.01.
Values may be sent and summed in bfloat16 or wider, within the bound.
A program may use at most 128 MiB of HBM per device.

```python
import math
import jax
import jax.numpy as jnp
import numpy as np
from jax import lax

D = 2048
HEADS = 8
KEY_DIM = 64
VALUE_DIM = 128
FFE = 3072
TOPK = 2
BLOCK = 64
ROWS_B = 256
QK_WIDTH = 512
V_WIDTH = 1024
EXPERTS = 32
TOKENS_A = 16384
TOKENS_B = 8192
NBLK = 256
CAP = 32
N_EP = 32
N_TP = 4


def draw_w_decay(key, part):
    limit = jnp.minimum(15.0 / jnp.sqrt(jnp.float32(D)), jnp.float32(1.0))
    entries = jax.random.normal(jax.random.fold_in(key, 11), (D, QK_WIDTH), jnp.float32) * (2.5 / jnp.sqrt(jnp.float32(D)))
    entries = jnp.clip(entries, -limit, limit)
    return entries.astype(jnp.bfloat16)


def draw_decay_bias(key, part):
    pick_key, slow_key, fast_key, block_key = jax.random.split(key, 4)
    slow_share = 0.5
    chosen = jax.random.uniform(pick_key, (QK_WIDTH,), jnp.float32) < slow_share
    slow_center = jnp.log(jnp.float32(0.86) * TOKENS_A)
    slow_base = slow_center + jax.random.uniform(slow_key, (QK_WIDTH,), jnp.float32, -0.5, 0.5)
    fast_base = jax.random.uniform(fast_key, (QK_WIDTH,), jnp.float32, -0.5, 1.5)
    channel_base = jnp.where(chosen, slow_base, fast_base)
    offset = jax.random.uniform(block_key, (NBLK, 1), jnp.float32, -0.8, 0.8)
    return (channel_base[None, :] + offset).astype(jnp.float32)


def block_scale(key, dims, pieces, smallest, high):
    level, own = 1.0, jax.random.fold_in(key, 6)
    for position, blocks in pieces:
        steps = jnp.exp(jax.random.uniform(jax.random.fold_in(own, position), (blocks,), jnp.float32, smallest / len(pieces), high / len(pieces)))
        level = level * jnp.repeat(steps, dims[position] // blocks).reshape([-1 if axis == position else 1 for axis in range(len(dims))])
    return level


def shared_out(own_key, own, number, rows, amount, top, bound, skew):
    order = jax.random.permutation(own_key, amount)
    crowded, common = portions_of(amount, rows * top, bound, skew, True), portions_of(amount, rows * top, bound, skew, False)
    places = jnp.arange(amount)

    def named(tallies, turn):
        used = int((tallies > 0).sum())
        fixed = max(1, used // 4)
        passed = fixed + (places - fixed + turn * (used - fixed)) % max(1, amount - fixed)
        return jnp.zeros((amount,), jnp.int32).at[order[jnp.where(places < fixed, places, passed)]].set(jnp.asarray(tallies, jnp.int32))

    tallies = jnp.where(number % 4 == 0, named(crowded, number // 4), named(common, number - number // 4 - 1))
    mixed = jax.random.permutation(jax.random.fold_in(own, 3), amount)
    source_of, taker = mixed[0:amount // 2 * 2:2], mixed[1:amount // 2 * 2:2]
    margin = jnp.minimum(tallies[source_of] - 1, bound - tallies[taker]) // 2
    margin = jnp.where((source_of == order[0]) | (taker == order[0]) | (tallies[taker] == 0), 0, jnp.maximum(margin, 0))
    passed = jax.random.randint(jax.random.fold_in(own, 4), (amount // 2,), 0, 1 << 20) % (margin + 1)
    tallies = tallies.at[source_of].add(-passed).at[taker].add(passed)
    labels = jnp.searchsorted(jnp.cumsum(tallies), jnp.arange(rows * top), side="right").astype(jnp.int32)
    grid = labels.reshape(top, rows).T
    grid = grid[jax.random.permutation(jax.random.fold_in(own, 1), rows)]
    turn = jax.random.randint(jax.random.fold_in(own, 2), (rows, 1), 0, top)
    return jnp.take_along_axis(grid, (jnp.arange(top)[None, :] + turn) % top, axis=1)


def portions_of(amount, total, reach, lean, full):
    loads = [(1 << 20) // math.isqrt(grade ** lean) + 1 for grade in range(1, amount + 1)]
    largest = reach if full else min(reach, max(-(-total // amount), total * loads[0] // sum(loads)))
    least = 1 if total - largest >= amount - 1 else 0
    holding, spare = [largest] + [least] * (amount - 1), total - largest - least * (amount - 1)
    while spare > 0:
        movable = [i for i in range(1, amount) if holding[i] < largest] or [i for i in range(1, amount) if holding[i] < reach]
        whole, budget = sum([loads[i] for i in movable]), spare
        for i in movable:
            extra = min(reach - holding[i], max(1, budget * loads[i] // whole), spare)
            holding[i] = holding[i] + extra
            spare = spare - extra
    return np.array(holding)


def gaussian(key, dims, spread, most, cuts=(), held_as=jnp.bfloat16):
    values = spread * jax.random.normal(key, dims, jnp.float32)
    if cuts:
        values = values * block_scale(key, dims, cuts, -0.22, 0.18)
    return jnp.clip(values, -most, most).astype(held_as)


def setup_inputs(seed: int = 0) -> dict:
    splits = jax.random.split(jax.random.key(seed), 18)
    tokens_first = gaussian(splits[0], (TOKENS_A, D), 1.0, 6.0, ((0, 32),))
    norm_gain_first = jnp.clip(1.0 + 0.18 * jax.random.normal(splits[1], (D,), jnp.float32), 0.1, 1.9)
    w_query = gaussian(splits[2], (D, QK_WIDTH), D ** -0.5, 0.125, ((1, 4),))
    w_key = gaussian(splits[3], (D, QK_WIDTH), D ** -0.5, 0.125, ((1, 4),))
    w_value = gaussian(splits[4], (D, V_WIDTH), D ** -0.5, 0.125, ((1, 4),))
    w_outgate = gaussian(splits[5], (D, V_WIDTH), D ** -0.5, 0.125, ((1, 4),))
    w_decay = draw_w_decay(jax.random.fold_in(splits[17], 71), 0)
    decay_bias = draw_decay_bias(jax.random.fold_in(splits[17], 71), 0)
    head_gain = jnp.clip(1.0 + 0.18 * jax.random.normal(splits[8], (V_WIDTH,), jnp.float32), 0.1, 1.9)
    w_mix_out = gaussian(splits[9], (V_WIDTH, D), V_WIDTH ** -0.5, 0.1875, ((0, 4),))
    tokens_second = gaussian(splits[10], (TOKENS_B, D), 1.0, 6.0, ((0, 32),))
    norm_gain_second = jnp.clip(1.0 + 0.18 * jax.random.normal(splits[11], (D,), jnp.float32), 0.1, 1.9)
    routes_keys = jax.random.split(jax.random.fold_in(splits[12], 1), TOKENS_B // ROWS_B)
    routes_turns = jax.random.permutation(jax.random.fold_in(splits[12], 3), TOKENS_B // ROWS_B)
    routes = jax.vmap(lambda own, number: shared_out(jax.random.fold_in(splits[12], 2), own, number, ROWS_B, EXPERTS, TOPK, CAP, 1))(routes_keys, routes_turns).reshape((TOKENS_B, TOPK))
    route_logits = gaussian(splits[13], (TOKENS_B, TOPK), 1.5, 8.0, ((0, 32),), jnp.float32)
    expert_gate = gaussian(splits[14], (EXPERTS, D, FFE), D ** -0.5, 0.125, ((0, 32), (2, 4)))
    expert_up = gaussian(splits[15], (EXPERTS, D, FFE), D ** -0.5, 0.125, ((0, 32), (2, 4)))
    expert_down = gaussian(splits[16], (EXPERTS, FFE, D), FFE ** -0.5, 0.109375, ((0, 32), (1, 4)))
    return dict(tokens_first=tokens_first, norm_gain_first=norm_gain_first, w_query=w_query, w_key=w_key, w_value=w_value, w_outgate=w_outgate, w_decay=w_decay, decay_bias=decay_bias, head_gain=head_gain, w_mix_out=w_mix_out, tokens_second=tokens_second, norm_gain_second=norm_gain_second, routes=routes, route_logits=route_logits, expert_gate=expert_gate, expert_up=expert_up, expert_down=expert_down)


EPS = 1e-06
TEMPER = 16.0

def rms_rows(rows_in, gain_row):
    wide_rows = rows_in.astype(jnp.float32)
    return wide_rows * lax.rsqrt(lax.optimization_barrier(jnp.mean(wide_rows * wide_rows, axis=-1, keepdims=True)) + EPS) * gain_row

def block_step(entry_state, inputs):
    queries, key_rows, value_matrix_rows, log_decay = inputs
    cumul_log = jnp.cumsum(log_decay, axis=0)
    forward_decay_rows = queries * jnp.exp(cumul_log)
    behind = key_rows * jnp.exp(-cumul_log)
    scores = jnp.einsum('thk,shk->hts', forward_decay_rows, behind, precision=lax.Precision.HIGHEST)
    block_len = queries.shape[0]
    causal = jnp.arange(block_len)[:, None] >= jnp.arange(block_len)[None, :]
    scores = jnp.where(causal[None], scores, jnp.zeros_like(scores))
    within = jnp.einsum('hts,shv->thv', scores, value_matrix_rows, precision=lax.Precision.HIGHEST)
    carried_state = jnp.einsum('azm,zmj->azj', forward_decay_rows, entry_state, precision=lax.Precision.HIGHEST)
    final_log_decay = cumul_log[-1]
    fading_factor = key_rows * jnp.exp(final_log_decay[None] - cumul_log)
    following_state = jnp.exp(final_log_decay)[:, :, None] * entry_state + jnp.einsum('drx,drm->rxm', fading_factor, value_matrix_rows, precision=lax.Precision.HIGHEST)
    return (following_state, within + carried_state)

def head_output(attended, out_gate, head_gain):
    scaled = attended * lax.rsqrt(lax.optimization_barrier(jnp.mean(attended * attended, axis=-1, keepdims=True)) + EPS)
    return (scaled.reshape(attended.shape[0], -1) * head_gain * jax.nn.silu(out_gate)).astype(jnp.bfloat16)

def reference(tokens_first, norm_gain_first, w_query, w_key, w_value, w_outgate, w_decay, decay_bias, head_gain, w_mix_out, tokens_second, norm_gain_second, routes, route_logits, expert_gate, expert_up, expert_down):
    normed = rms_rows(tokens_first, norm_gain_first).astype(jnp.bfloat16)
    queries = (jnp.dot(normed, w_query, preferred_element_type=jnp.float32) * KEY_DIM ** (-0.5)).astype(jnp.bfloat16)
    key_rows = jnp.dot(normed, w_key, preferred_element_type=jnp.float32).astype(jnp.bfloat16)
    value_matrix_rows = jnp.dot(normed, w_value, preferred_element_type=jnp.float32).astype(jnp.bfloat16)
    out_gate = jnp.dot(normed, w_outgate, preferred_element_type=jnp.float32)
    decay_pre = jnp.dot(normed, w_decay, preferred_element_type=jnp.float32).reshape(NBLK, BLOCK, QK_WIDTH) + decay_bias[:, None, :]
    log_decay = (jax.nn.log_sigmoid(decay_pre) / TEMPER).reshape(NBLK, BLOCK, HEADS, KEY_DIM)
    queries, key_rows, value_matrix_rows = lax.optimization_barrier((queries, key_rows, value_matrix_rows))
    query_wide = queries.astype(jnp.float32).reshape(NBLK, BLOCK, HEADS, KEY_DIM)
    key_wide = key_rows.astype(jnp.float32).reshape(NBLK, BLOCK, HEADS, KEY_DIM)
    value_wide = value_matrix_rows.astype(jnp.float32).reshape(NBLK, BLOCK, HEADS, VALUE_DIM)
    start_state = jnp.zeros((HEADS, KEY_DIM, VALUE_DIM), jnp.float32)
    _, attended = lax.scan(block_step, start_state, (query_wide, key_wide, value_wide, log_decay))
    attended = attended.reshape(TOKENS_A, HEADS, VALUE_DIM)
    gated_rows = head_output(attended, out_gate, head_gain)
    mixed_first = jnp.dot(gated_rows, w_mix_out, preferred_element_type=jnp.float32).astype(jnp.bfloat16)
    normed_second = rms_rows(tokens_second, norm_gain_second).astype(jnp.bfloat16)
    flat_routes = routes.reshape(-1)
    copies = flat_routes.shape[0]
    slot_room = N_EP * CAP

    def expert_rows(expert_id, collected):
        copy_index = jnp.nonzero(flat_routes == expert_id, size=slot_room, fill_value=copies)[0]
        picked_rows = jnp.take(normed_second, copy_index // TOPK, axis=0, mode='clip')
        gate_out = jnp.dot(picked_rows, expert_gate[expert_id], preferred_element_type=jnp.float32)
        up_out = jnp.dot(picked_rows, expert_up[expert_id], preferred_element_type=jnp.float32)
        hidden = (jax.nn.silu(gate_out) * up_out).astype(jnp.bfloat16)
        hidden_wide = hidden.reshape(slot_room, N_TP, FFE // N_TP).astype(jnp.float32)
        down_wide = expert_down[expert_id].reshape(N_TP, FFE // N_TP, D).astype(jnp.float32)
        tp_parts = jnp.einsum('mtf,tfd->tmd', hidden_wide, down_wide).astype(jnp.bfloat16)
        tp_parts = lax.optimization_barrier(tp_parts).astype(jnp.float32)
        result = lax.optimization_barrier(jnp.sum(tp_parts, axis=0)).astype(jnp.bfloat16)
        return collected.at[copy_index].set(result, mode='drop')
    collected = lax.fori_loop(0, EXPERTS, expert_rows, jnp.zeros((copies, D), jnp.bfloat16))
    route_share = jax.nn.sigmoid(route_logits - route_logits[:, ::-1])
    picked = collected.reshape(TOKENS_B, TOPK, D).astype(jnp.float32)
    mixed_second = lax.optimization_barrier(jnp.sum(picked * route_share[:, :, None], axis=1)).astype(jnp.bfloat16)
    return (mixed_first, mixed_second)
```

```python
import jax
import jax.numpy as jnp
from jax import lax
from jax.experimental import pallas as pl
from jax.experimental.pallas import tpu as pltpu
from jax.sharding import PartitionSpec as P

KEY_DIM = 64
VALUE_DIM = 128
BLOCK = 64
CAP = 32
EPS = 1e-06
TEMPER = 16.0
NZ, NY, NC = 4, 4, 2
MESH = pl.DeviceIdType.MESH
HIGH = lax.Precision.HIGHEST
F32, BF16 = jnp.float32, jnp.bfloat16

ORDER = [
    (0, 0, 0), (0, 0, 1),
    (0, 1, 0), (1, 0, 0), (0, 3, 0), (3, 0, 0), (0, 2, 0), (2, 0, 0),
    (0, 1, 1), (1, 0, 1), (0, 3, 1), (3, 0, 1), (0, 2, 1), (2, 0, 1), (1, 1, 0), (3, 3, 0),
    (1, 3, 0), (3, 1, 0), (1, 1, 1), (3, 3, 1), (1, 2, 0), (2, 1, 0), (3, 2, 0), (2, 3, 0),
    (1, 3, 1), (3, 1, 1), (2, 2, 0), (1, 2, 1), (2, 1, 1), (3, 2, 1), (2, 3, 1), (2, 2, 1),
]
CHUNKS = 4
PER = 8


def dot(a, b, precision=None):
    return jnp.dot(a, b, preferred_element_type=F32, precision=precision)


def dot_t0(a, b, precision=None):
    return lax.dot_general(
        a, b, (((0,), (0,)), ((), ())), preferred_element_type=F32, precision=precision
    )


def dot_t1(a, b, precision=None):
    return lax.dot_general(
        a, b, (((1,), (1,)), ((), ())), preferred_element_type=F32, precision=precision
    )


def iota(shape, dim):
    return lax.broadcasted_iota(jnp.int32, shape, dim)


def rms(rows, gain):
    wide = rows.astype(F32)
    return wide * lax.rsqrt(jnp.mean(wide * wide, axis=-1, keepdims=True) + EPS) * gain


def log_sigmoid(x):
    return jnp.minimum(x, 0.0) - jnp.log1p(jnp.exp(-jnp.abs(x)))


def kernel(
    tok1_h, g1_ref, wq_h, wk_h, wv_h, wo_h, wd_h, bias_ref, hgain_ref, wmix_h,
    tok2_h, g2_ref, routes_ref, routes_t_ref, logits_ref, wg_h, wu_h, wdn_h,
    out1_ref, out2_ref,
    tok2, norm2, send2, recv2, tok1, norm1, w1, wmix, wg, wu, wdn, proj, att, reach,
    sbd, total, msg, pmsg, inc, joint, psend, prs, rsend, rret, mpart, mrecv, hid, chmsg, chrecv,
    ld, dsend, drecv, rs_ssem, rs_rsem, mx_ssem, mx_rsem, rt_ssem, rt_rsem,
    dd_ssem, dd_rsem, ch_ssem, ch_rsem,
):
    ep, tp = lax.axis_index("ep"), lax.axis_index("tp")
    z, y, c = ep // (NY * NC), (ep // NC) % NY, ep % NC
    chip = z * NY + y

    def target(o, sign=1):
        dz, dy, dc = o
        return (
            ((z + sign * dz + NZ) % NZ) * (NY * NC)
            + ((y + sign * dy + NY) % NY) * NC
            + (c + dc) % NC
        )

    def remote(src, dst, ssem, rsem, to_ep, to_tp):
        return pltpu.make_async_remote_copy(
            src_ref=src, dst_ref=dst, send_sem=ssem, recv_sem=rsem,
            device_id=(to_ep, to_tp), device_id_type=MESH,
        )

    loads = [
        (tok2_h, tok2), (tok1_h, tok1),
        (wq_h, w1.at[:, 0:128]), (wk_h, w1.at[:, 128:256]), (wv_h, w1.at[:, 256:512]),
        (wo_h, w1.at[:, 512:768]), (wd_h, w1.at[:, 768:896]),
        (wg_h.at[0], wg), (wu_h.at[0], wu), (wdn_h.at[0], wdn), (wmix_h, wmix),
    ]
    loads = [pltpu.make_async_copy(s, d, ld.at[i]) for i, (s, d) in enumerate(loads)]
    for cp in loads:
        cp.start()

    barrier = pltpu.get_barrier_semaphore()
    for o in ORDER[1:]:
        pl.semaphore_signal(barrier, inc=1, device_id=(target(o), tp), device_id_type=MESH)
    for d in range(1, 4):
        pl.semaphore_signal(barrier, inc=1, device_id=(ep, (tp + d) % 4), device_id_type=MESH)

    rows2 = norm2.shape[0]
    experts = send2.shape[0]
    r0t, r1t = routes_t_ref[0:1, :], routes_t_ref[1:2, :]
    e_sub = iota((experts, rows2), 0)
    member_t = ((r0t == e_sub) | (r1t == e_sub)).astype(F32)
    before_t = (iota((rows2, rows2), 0) < iota((rows2, rows2), 1)).astype(BF16)
    rank_t = dot(member_t.astype(BF16), before_t)
    place_t = jnp.where(member_t > 0.0, rank_t, -1.0)
    loads[0].wait()
    norm2[...] = rms(tok2[...], g2_ref[...]).astype(BF16)
    for g in range(experts // 8):
        place = place_t[8 * g : 8 * g + 8]
        want = iota((8, CAP, rows2), 1).astype(F32)
        pick = (place[:, None, :] == want).astype(BF16).reshape(8 * CAP, rows2)
        for n in range(norm2.shape[1] // 512):
            cols = slice(512 * n, 512 * n + 512)
            send2[8 * g : 8 * g + 8, :, cols] = (
                dot(pick, norm2[:, cols]).astype(BF16).reshape(8, CAP, 512)
            )
    pl.semaphore_wait(barrier, len(ORDER) - 1 + 3)

    def dispatch(s):
        to = target(ORDER[s])
        remote(send2.at[to], recv2.at[s], dsend, drecv.at[s // PER], to, tp).start()

    for s in range(1, 16):
        dispatch(s)
    recv2[0] = send2[ep]

    loads[1].wait()
    for i in range(tok1.shape[0] // 128):
        rows = slice(128 * i, 128 * i + 128)
        norm1[rows, :] = rms(tok1[rows, :], g1_ref[...]).astype(BF16)
    for i in range(2, 7):
        loads[i].wait()
    for lo, hi in ((0, 256), (256, 512), (512, 768), (768, 896)):
        proj[:, lo:hi] = dot(norm1[...], w1[:, lo:hi])
    sbd[...] = jnp.zeros_like(sbd)
    total[...] = jnp.zeros_like(total)
    own_head = (iota(sbd.shape, 0) // KEY_DIM == iota(sbd.shape, 1) // VALUE_DIM).astype(F32)
    tri = (iota((BLOCK, BLOCK), 0) >= iota((BLOCK, BLOCK), 1)).astype(F32)
    head_lane = iota((BLOCK, 2 * KEY_DIM), 1) // KEY_DIM

    def block(b, _):
        rows = pl.ds(pl.multiple_of(b * BLOCK, BLOCK), BLOCK)
        query = (proj[rows, 0:128] * KEY_DIM ** (-0.5)).astype(BF16).astype(F32)
        key = proj[rows, 128:256].astype(BF16).astype(F32)
        value = proj[rows, 256:512].astype(BF16).astype(F32)
        log_decay = log_sigmoid(proj[rows, 768:896] + bias_ref[pl.ds(b, 1), :]) / TEMPER
        cumul = dot(tri, log_decay, HIGH)
        final = cumul[BLOCK - 1 : BLOCK, :]
        forward = query * jnp.exp(cumul)
        behind = key * jnp.exp(-cumul)
        fading = key * jnp.exp(final - cumul)
        within = []
        for h in range(2):
            mine = jnp.where(head_lane == h, forward, 0.0)
            scores = dot_t1(mine, behind, HIGH)
            scores = jnp.where(tri > 0.0, scores, 0.0)
            within.append(dot(scores, value[:, VALUE_DIM * h : VALUE_DIM * (h + 1)], HIGH))
        att[rows, :] = jnp.concatenate(within, axis=1) + dot(forward, sbd[...], HIGH)
        fall = dot_t0(log_decay, jnp.ones((BLOCK, sbd.shape[1]), F32), HIGH)
        sbd[...] = jnp.exp(fall) * sbd[...] + own_head * dot_t0(fading, value, HIGH)
        reach[rows, :] = query * jnp.exp(cumul + total[0:1, :])
        total[0:1, :] = total[0:1, :] + final
        return 0

    lax.fori_loop(0, proj.shape[0] // BLOCK, block, 0)
    msg[0:64, :] = sbd[0:64, 0:128]
    msg[64:128, :] = sbd[64:128, 128:256]
    msg[128:136, :] = total[...]
    partner = ep + 1 - 2 * c
    first = remote(msg, pmsg, dd_ssem.at[0], dd_rsem.at[0], partner, tp)
    first.start()

    def column(row8):
        return jnp.exp(dot_t0(row8, jnp.ones((8, 128), F32), HIGH))

    def expert(j):
        x_rows = recv2[PER * j : PER * j + PER].reshape(PER * CAP, recv2.shape[2])
        for n in range(hid.shape[1] // 256):
            cols = slice(256 * n, 256 * n + 256)
            gate = dot(x_rows, wg[:, cols])
            up = dot(x_rows, wu[:, cols])
            hid[:, cols] = (gate * jax.nn.sigmoid(gate) * up).astype(BF16)
        for d in (1, 3, 2, 0):
            t = (tp + d) % 4
            cols = pl.ds(pl.multiple_of(t * 512, 512), 512)
            psend[j, d] = dot(hid[...], wdn[:, cols]).astype(BF16)
            if d:
                remote(psend.at[j, d], prs.at[j, d - 1], rs_ssem, rs_rsem.at[j], ep, t).start()

    def reduce(j):
        remote(prs.at[j], prs.at[j], rs_ssem, rs_rsem.at[j], ep, tp).wait_recv()
        whole = psend[j, 0].astype(F32)
        for d in range(3):
            whole = whole + prs[j, d].astype(F32)
        rsend[j] = whole.astype(BF16).reshape(PER, CAP, 512)
        for i in range(PER):
            s = PER * j + i
            if s == 0:
                rret[ep] = rsend[0, 0]
            else:
                to = target(ORDER[s], -1)
                remote(rsend.at[j, i], rret.at[ep], rt_ssem, rt_rsem, to, tp).start()

    def arrived(j):
        part = recv2.at[1:PER] if j == 0 else recv2.at[PER * j : PER * j + PER]
        remote(part, part, dsend, drecv.at[j], ep, tp).wait_recv()

    first.wait_recv()
    later_core = c == 1
    mine, other = msg[0:128, :], pmsg[0:128, :]
    older = jnp.where(later_core, other, mine)
    newer = jnp.where(later_core, mine, other)
    newer_total = jnp.where(later_core, msg[128:136, :], pmsg[128:136, :])
    joint[...] = column(newer_total) * older + newer
    half = pl.ds(pl.multiple_of(c * 64, 64), 64)
    chmsg[0:64, :] = joint[half, :]
    chmsg[64:72, :] = msg[128:136, :] + pmsg[128:136, :]
    hops = [(dz, dy) for dz in range(NZ) for dy in range(NY) if (dz, dy) != (0, 0)]

    def share(k):
        to = target((*hops[k], 0))
        return to // NC, remote(chmsg, chrecv.at[chip], ch_ssem.at[k], ch_rsem.at[chip], to, tp)

    for k in range(len(hops)):
        to_chip, cp = share(k)
        pl.when(to_chip > chip)(cp.start)
    for s in range(16, 32):
        dispatch(s)

    for i in range(7, 11):
        loads[i].wait()
    arrived(0)
    expert(0)
    arrived(1)
    expert(1)

    inc[half, :] = jnp.zeros((64, 128), F32)

    def join(k, _):
        cp = remote(chrecv.at[k], chrecv.at[k], ch_ssem.at[0], ch_rsem.at[k], ep, tp)
        cp.wait_recv()
        fade = column(chrecv[k, 64:72, :])
        inc[half, :] = jnp.where(later_core, fade[64:128], fade[0:64]) * inc[half, :] + chrecv[k, 0:64, :]
        return 0

    lax.fori_loop(0, chip, join, 0)
    second = remote(inc.at[half], inc.at[half], dd_ssem.at[1], dd_rsem.at[1], partner, tp)
    second.start()
    reduce(0)
    second.wait()
    joined = column(pmsg[128:136, :]) * inc[...] + pmsg[0:128, :]
    entry = jnp.where(later_core, joined, inc[...])
    entry_bd = jnp.concatenate([entry, entry], axis=1) * own_head
    for i in range(att.shape[0] // 128):
        rows = slice(128 * i, 128 * i + 128)
        whole = att[rows, :] + dot(reach[rows, :], entry_bd, HIGH)
        parts = []
        for h in range(2):
            one = whole[:, VALUE_DIM * h : VALUE_DIM * (h + 1)]
            parts.append(one * lax.rsqrt(jnp.mean(one * one, axis=-1, keepdims=True) + EPS))
        out_gate = proj[rows, 512:768]
        gated = jnp.concatenate(parts, axis=1) * hgain_ref[...] * (out_gate * jax.nn.sigmoid(out_gate))
        mpart[rows, :] = dot(gated.astype(BF16), wmix[...]).astype(BF16)
    quarter = out1_ref.shape[0]
    for d in (1, 3, 2):
        t = (tp + d) % 4
        rows = pl.ds(pl.multiple_of(t * quarter, quarter), quarter)
        remote(mpart.at[rows], mrecv.at[d - 1], mx_ssem, mx_rsem, ep, t).start()

    arrived(2)
    expert(2)
    reduce(1)
    arrived(3)
    expert(3)
    reduce(2)
    remote(mrecv, mrecv, mx_ssem, mx_rsem, ep, tp).wait_recv()
    rows = pl.ds(pl.multiple_of(tp * quarter, quarter), quarter)
    whole = mpart[rows, :].astype(F32)
    for d in range(3):
        whole = whole + mrecv[d].astype(F32)
    out1_ref[...] = whole.astype(BF16)
    reduce(3)

    e_lane = iota((rows2, experts), 1)
    r_cols = [routes_ref[:, 0:1], routes_ref[:, 1:2]]
    member = ((r_cols[0] == e_lane) | (r_cols[1] == e_lane)).astype(BF16)
    earlier = (iota((rows2, rows2), 0) > iota((rows2, rows2), 1)).astype(BF16)
    rank = dot(earlier, member)
    spread = iota((rows2, experts * CAP), 1).astype(F32)
    picks = []
    for r in range(2):
        slot = jnp.sum(jnp.where(r_cols[r] == e_lane, rank, 0.0), axis=1, keepdims=True)
        place = slot + (r_cols[r] * CAP).astype(F32)
        picks.append((spread == place).astype(BF16))
    remote(rret.at[1:experts], rret.at[1:experts], rt_ssem, rt_rsem, ep, tp).wait_recv()
    flat = rret[...].reshape(experts * CAP, 512)
    mixed = jnp.zeros((rows2, 512), F32)
    for r in range(2):
        share_r = jax.nn.sigmoid(logits_ref[:, r : r + 1] - logits_ref[:, 1 - r : 2 - r])
        mixed = mixed + dot(picks[r], flat) * share_r
    out2_ref[...] = mixed.astype(BF16)

    remote(send2.at[1:experts], send2.at[1:experts], dsend, drecv.at[0], ep, tp).wait_send()
    for j in range(CHUNKS):
        remote(prs.at[j], prs.at[j], rs_ssem, rs_rsem.at[j], ep, tp).wait_send()
    remote(mrecv, mrecv, mx_ssem, mx_rsem, ep, tp).wait_send()
    remote(rret.at[1:experts], rret.at[1:experts], rt_ssem, rt_rsem, ep, tp).wait_send()
    first.wait_send()
    for k in range(len(hops)):
        to_chip, cp = share(k)
        pl.when(to_chip > chip)(cp.wait_send)


def body(
    tokens_first, norm_gain_first, w_query, w_key, w_value, w_outgate, w_decay, decay_bias,
    head_gain, w_mix_out, tokens_second, norm_gain_second, routes, route_logits,
    expert_gate, expert_up, expert_down,
):
    hbm, vmem = pl.BlockSpec(memory_space=pl.ANY), pl.BlockSpec(memory_space=pltpu.VMEM)
    rows1, width = tokens_first.shape
    rows2 = tokens_second.shape[0]
    hidden = expert_gate.shape[2]
    experts = NZ * NY * NC
    quarter = width // 4
    V, D = pltpu.VMEM, pltpu.SemaphoreType.DMA
    return pl.pallas_call(
        kernel,
        out_shape=(
            jax.ShapeDtypeStruct((rows1 // 4, width), BF16),
            jax.ShapeDtypeStruct((rows2, quarter), BF16),
        ),
        in_specs=[
            hbm, vmem, hbm, hbm, hbm, hbm, hbm, vmem, vmem, hbm,
            hbm, vmem, vmem, vmem, vmem, hbm, hbm, hbm,
        ],
        out_specs=(vmem, vmem),
        scratch_shapes=[
            V((rows2, width), BF16), V((rows2, width), BF16),
            V((experts, CAP, width), BF16), V((experts, CAP, width), BF16),
            V((rows1, width), BF16), V((rows1, width), BF16),
            V((width, 896), BF16), V((256, width), BF16),
            V((width, hidden), BF16), V((width, hidden), BF16), V((hidden, width), BF16),
            V((rows1, 896), F32), V((rows1, 256), F32), V((rows1, 128), F32),
            V((128, 256), F32), V((8, 128), F32), V((136, 128), F32), V((136, 128), F32),
            V((128, 128), F32), V((128, 128), F32),
            V((CHUNKS, 4, PER * CAP, quarter), BF16), V((CHUNKS, 3, PER * CAP, quarter), BF16),
            V((CHUNKS, PER, CAP, quarter), BF16), V((experts, CAP, quarter), BF16),
            V((rows1, width), BF16), V((3, rows1 // 4, width), BF16),
            V((PER * CAP, hidden), BF16), V((72, 128), F32), V((NZ * NY, 72, 128), F32),
            D((11,)), D(()), D((CHUNKS,)), D(()), D((CHUNKS,)), D(()), D(()), D(()), D(()),
            D((2,)), D((2,)), D((15,)), D((16,)),
        ],
        compiler_params=pltpu.CompilerParams(
            collective_id=0, has_side_effects=True, vmem_limit_bytes=63 * 2**20
        ),
        name="layer",
    )(
        tokens_first, norm_gain_first.reshape(1, -1), w_query, w_key, w_value, w_outgate, w_decay,
        decay_bias, head_gain.reshape(1, -1), w_mix_out, tokens_second,
        norm_gain_second.reshape(1, -1), routes, routes.T, route_logits,
        expert_gate, expert_up, expert_down,
    )


def solution(mesh):
    ep_tp = ("ep", "tp")
    in_specs = (
        P("ep", None), P(), P(None, "tp"), P(None, "tp"), P(None, "tp"), P(None, "tp"),
        P(None, "tp"), P("ep", "tp"), P("tp"), P("tp", None), P("ep", None), P(), P("ep", None),
        P("ep", None), P("ep", None, "tp"), P("ep", None, "tp"), P("ep", "tp", None),
    )
    out_specs = (P(ep_tp, None), P("ep", "tp"))
    return jax.shard_map(body, mesh=mesh, in_specs=in_specs, out_specs=out_specs, check_vma=False)
```

```python
import jax
import jax.numpy as jnp
from jax import lax
from jax.experimental import pallas as pl
from jax.experimental.pallas import tpu as pltpu
from jax.sharding import PartitionSpec as P

KEY_DIM = 64
VALUE_DIM = 128
BLOCK = 64
CAP = 32
EPS = 1e-06
TEMPER = 16.0
NZ, NY, NC = 4, 4, 2
MESH = pl.DeviceIdType.MESH
HIGH = lax.Precision.HIGHEST
F32, BF16 = jnp.float32, jnp.bfloat16

NEAR, FAR = (1, 3), (2,)
ORDER = (
    [(0, 0, 0), (0, 0, 1)]
    + [o for d in NEAR for o in ((d, 0, 0), (0, d, 0))]
    + [(dz, dy, c) for dz in NEAR for dy in NEAR for c in (0, 1)]
    + [o for c in (0, 1) for o in ((2, 0, c), (0, 2, c))]
    + [o for d in NEAR for o in ((d, 2, 0), (2, d, 1))]
    + [o for d in NEAR for o in ((2, d, 0), (d, 2, 1))]
    + [(2, 2, 0), (2, 2, 1)]
    + [o for d in NEAR for o in ((d, 0, 1), (0, d, 1))]
)
SLOT = {o: s for s, o in enumerate(ORDER)}
SIZES = (6, 8, 8, 6, 4)
START = [sum(SIZES[:j]) for j in range(len(SIZES))]
CHUNKS = len(SIZES)


def dot(a, b, precision=None):
    return jnp.dot(a, b, preferred_element_type=F32, precision=precision)


def dot_t0(a, b, precision=None):
    return lax.dot_general(
        a, b, (((0,), (0,)), ((), ())), preferred_element_type=F32, precision=precision
    )


def dot_t1(a, b, precision=None):
    return lax.dot_general(
        a, b, (((1,), (1,)), ((), ())), preferred_element_type=F32, precision=precision
    )


def iota(shape, dim):
    return lax.broadcasted_iota(jnp.int32, shape, dim)


def rms(rows, gain):
    wide = rows.astype(F32)
    return wide * lax.rsqrt(jnp.mean(wide * wide, axis=-1, keepdims=True) + EPS) * gain


def log_sigmoid(x):
    return jnp.minimum(x, 0.0) - jnp.log1p(jnp.exp(-jnp.abs(x)))


def kernel(
    tok1_h, g1_ref, wq_h, wk_h, wv_h, wo_h, wd_h, bias_ref, hgain_ref, wmix_h,
    tok2_h, g2_ref, routes_t_ref, logits_t_ref, wg_h, wu_h, wdn_h,
    out1_ref, out2_ref,
    tok2, norm2, send2, recv2, relay, tok1, norm1, w1, wfull, wg, wu, wdn, proj, att, reach,
    sbd, total, msg, pmsg, inc, joint, psend, r1, s2, r2, rsend, rret, gated, spread, pickm, hid,
    chmsg, ymsg, zmsg, yrecv, zrecv,
    ld, dsend, drecv, hand_sem, rs_ssem, r1_rsem, r2_rsem, w_ssem, w_rsem, mx_ssem, mx_rsem, rt_ssem, rt_rsem,
    dd_ssem, dd_rsem, ch_ssem, y_rsem, zm_ssem, z_rsem,
):
    ep, tp = lax.axis_index("ep"), lax.axis_index("tp")
    z, y, c = ep // (NY * NC), (ep // NC) % NY, ep % NC
    chip = z * NY + y
    flips = (tp, tp + 1 - 2 * (tp % 2), (tp + 2) % 4, 3 - tp)
    partner = ep + 1 - 2 * c

    def target(o, sign=1):
        dz, dy, dc = o
        return (
            ((z + sign * dz + NZ) % NZ) * (NY * NC)
            + ((y + sign * dy + NY) % NY) * NC
            + (c + dc) % NC
        )

    def remote(src, dst, ssem, rsem, to_ep, to_tp):
        return pltpu.make_async_remote_copy(
            src_ref=src, dst_ref=dst, send_sem=ssem, recv_sem=rsem,
            device_id=(to_ep, to_tp), device_id_type=MESH,
        )

    loads = [
        (tok2_h, tok2), (tok1_h, tok1),
        (wq_h, w1.at[:, 0:128]), (wk_h, w1.at[:, 128:256]), (wv_h, w1.at[:, 256:512]),
        (wo_h, w1.at[:, 512:768]), (wd_h, w1.at[:, 768:896]),
        (wg_h.at[0], wg), (wu_h.at[0], wu), (wdn_h.at[0], wdn),
        (wmix_h, wfull.at[pl.ds(pl.multiple_of(tp * 256, 256), 256)]),
    ]
    loads = [pltpu.make_async_copy(s, d, ld.at[i]) for i, (s, d) in enumerate(loads)]
    for cp in loads:
        cp.start()

    barrier = pltpu.get_barrier_semaphore()
    for o in ORDER[1:]:
        pl.semaphore_signal(barrier, inc=1, device_id=(target(o), tp), device_id_type=MESH)
    for d in range(1, 4):
        pl.semaphore_signal(barrier, inc=1, device_id=(ep, (tp + d) % 4), device_id_type=MESH)

    rows2 = norm2.shape[0]
    experts = send2.shape[0]
    r0t, r1t = routes_t_ref[0:1, :], routes_t_ref[1:2, :]
    e_sub = iota((experts, rows2), 0)
    gap = logits_t_ref[0:1, :] - logits_t_ref[1:2, :]
    share_t = jnp.concatenate([jax.nn.sigmoid(gap), jax.nn.sigmoid(-gap)], axis=0)
    member_t = ((r0t == e_sub) | (r1t == e_sub)).astype(F32)
    before_t = (iota((rows2, rows2), 0) < iota((rows2, rows2), 1)).astype(BF16)
    rank_t = dot(member_t.astype(BF16), before_t)
    place_t = jnp.where(member_t > 0.0, rank_t, -1.0)
    loads[0].wait()
    norm2[...] = rms(tok2[...], g2_ref[...]).astype(BF16)
    for g in range(experts // 8):
        place = place_t[8 * g : 8 * g + 8]
        want = iota((8, CAP, rows2), 1).astype(F32)
        pick = (place[:, None, :] == want).astype(BF16).reshape(8 * CAP, rows2)
        for n in range(norm2.shape[1] // 512):
            cols = slice(512 * n, 512 * n + 512)
            send2[8 * g : 8 * g + 8, :, cols] = (
                dot(pick, norm2[:, cols]).astype(BF16).reshape(8, CAP, 512)
            )
    pl.semaphore_wait(barrier, len(ORDER) - 1 + 3)

    def straight(o):
        to, s = target(o), SLOT[o]
        remote(send2.at[to], recv2.at[s], dsend, drecv.at[s], to, tp).start()

    def turn(o):
        dz, dy, dc = o
        corner = target((0, dy, 1) if dc else (dz, 0, 0))
        onward = target((dz, 0, 0) if dc else (0, dy, 0))
        k = (dc * 3 + dz - 1) * 3 + dy - 1
        into = remote(send2.at[target(o)], relay.at[k], dsend, hand_sem.at[k], corner, tp)
        s = SLOT[o]
        out = remote(relay.at[k], recv2.at[s], dsend, drecv.at[s], onward, tp)
        return into, out

    def leave(dzs, dys):
        for dz in dzs:
            for dy in dys:
                turn((dz, dy, 0))[0].start()
                turn((dy, dz, 1))[0].start()

    def pass_on(dzs, dys):
        for dz in dzs:
            for dy in dys:
                for o in ((dz, dy, 0), (dy, dz, 1)):
                    into, out = turn(o)
                    into.wait_recv()
                    out.start()

    leave(NEAR, NEAR)
    straight((0, 0, 1))
    for d in NEAR:
        straight((d, 0, 0))
        straight((0, d, 0))
    leave(NEAR, FAR)
    leave(FAR, NEAR)
    leave(FAR, FAR)

    def shard_rows(t, core, lo, n):
        start = t * 256 + core * 128 + lo
        return pl.ds(pl.multiple_of(start, 64), n)

    def hand_on(owner, lo, n, k, to_ep, to_tp):
        rows = shard_rows(owner, c, lo, n)
        remote(wfull.at[rows], wfull.at[rows], w_ssem, w_rsem.at[k], to_ep, to_tp).start()

    def handed(n, k):
        remote(wfull.at[0:n], wfull.at[0:n], w_ssem, w_rsem.at[k], ep, tp).wait_recv()

    loads[10].wait()
    hand_on(tp, 0, 64, 0, ep, flips[1])
    hand_on(tp, 64, 64, 1, ep, flips[3])
    recv2[0] = send2[ep]

    loads[1].wait()
    for i in range(tok1.shape[0] // 128):
        rows = slice(128 * i, 128 * i + 128)
        norm1[rows, :] = rms(tok1[rows, :], g1_ref[...]).astype(BF16)
    for i in range(2, 7):
        loads[i].wait()
    for lo, hi in ((0, 256), (256, 512), (512, 768), (768, 896)):
        proj[:, lo:hi] = dot(norm1[...], w1[:, lo:hi])
    sbd[...] = jnp.zeros_like(sbd)
    total[...] = jnp.zeros_like(total)
    own_head = (iota(sbd.shape, 0) // KEY_DIM == iota(sbd.shape, 1) // VALUE_DIM).astype(F32)
    tri = (iota((BLOCK, BLOCK), 0) >= iota((BLOCK, BLOCK), 1)).astype(F32)
    head_lane = iota((BLOCK, 2 * KEY_DIM), 1) // KEY_DIM

    def block(b, _):
        rows = pl.ds(pl.multiple_of(b * BLOCK, BLOCK), BLOCK)
        query = (proj[rows, 0:128] * KEY_DIM ** (-0.5)).astype(BF16).astype(F32)
        key = proj[rows, 128:256].astype(BF16).astype(F32)
        value = proj[rows, 256:512].astype(BF16).astype(F32)
        log_decay = log_sigmoid(proj[rows, 768:896] + bias_ref[pl.ds(b, 1), :]) / TEMPER
        cumul = dot(tri, log_decay, HIGH)
        final = cumul[BLOCK - 1 : BLOCK, :]
        forward = query * jnp.exp(cumul)
        behind = key * jnp.exp(-cumul)
        fading = key * jnp.exp(final - cumul)
        within = []
        for h in range(2):
            mine = jnp.where(head_lane == h, forward, 0.0)
            scores = dot_t1(mine, behind, HIGH)
            scores = jnp.where(tri > 0.0, scores, 0.0)
            within.append(dot(scores, value[:, VALUE_DIM * h : VALUE_DIM * (h + 1)], HIGH))
        att[rows, :] = jnp.concatenate(within, axis=1) + dot(forward, sbd[...], HIGH)
        fall = dot_t0(log_decay, jnp.ones((BLOCK, sbd.shape[1]), F32), HIGH)
        sbd[...] = jnp.exp(fall) * sbd[...] + own_head * dot_t0(fading, value, HIGH)
        reach[rows, :] = query * jnp.exp(cumul + total[0:1, :])
        total[0:1, :] = total[0:1, :] + final
        return 0

    blocks = proj.shape[0] // BLOCK
    lax.fori_loop(0, blocks // 2, block, 0)
    handed(64, 0)
    hand_on(tp, 0, 64, 2, ep, flips[3])
    hand_on(flips[1], 0, 64, 2, ep, flips[3])
    handed(64, 1)
    hand_on(tp, 64, 64, 3, ep, flips[1])
    hand_on(flips[3], 64, 64, 3, ep, flips[1])
    pass_on(NEAR, NEAR)
    lax.fori_loop(blocks // 2, blocks, block, 0)
    msg[0:64, :] = sbd[0:64, 0:128]
    msg[64:128, :] = sbd[64:128, 128:256]
    msg[128:136, :] = total[...]
    first = remote(msg, pmsg, dd_ssem.at[0], dd_rsem.at[0], partner, tp)
    first.start()

    def column(row8):
        return jnp.exp(dot_t0(row8, jnp.ones((8, 128), F32), HIGH))

    def rows_of(j, p=None):
        lo, n = START[j] * CAP, SIZES[j] * CAP
        return slice(lo, lo + n) if p is None else slice(lo + p * n // 2, lo + (p + 1) * n // 2)

    def expert(j):
        n = SIZES[j]
        x_rows = recv2[START[j] : START[j] + n].reshape(n * CAP, recv2.shape[2])
        for lo in range(0, hid.shape[1], 256):
            cols = slice(lo, lo + 256)
            gate = dot(x_rows, wg[:, cols])
            up = dot(x_rows, wu[:, cols])
            hid[0 : n * CAP, cols] = (gate * jax.nn.sigmoid(gate) * up).astype(BF16)
        for m in (2, 1, 3, 0):
            cols = pl.ds(pl.multiple_of(flips[m] * 512, 512), 512)
            psend[m, rows_of(j), :] = dot(hid[0 : n * CAP, :], wdn[:, cols]).astype(BF16)
            for p, q, k in ((0, 1, 0), (0, 2, 1), (1, 3, 0), (1, 2, 1)):
                if q == m:
                    remote(
                        psend.at[m, rows_of(j, p)], r1.at[k, rows_of(j, p)],
                        rs_ssem, r1_rsem.at[j, p], ep, flips[1 + 2 * p],
                    ).start()

    def middle(j):
        for p in range(2):
            rows = rows_of(j, p)
            both = r1.at[:, rows]
            remote(both, both, rs_ssem, r1_rsem.at[j, p], ep, tp).wait_recv()
            pair = psend[3 - 2 * p, rows, :].astype(F32) + r1[1, rows, :].astype(F32)
            s2[rows, :] = pair.astype(BF16)
            remote(s2.at[rows], r2.at[rows], rs_ssem, r2_rsem.at[j, p], ep, flips[3 - 2 * p]).start()

    def reduce(j):
        for p in range(2):
            rows = rows_of(j, p)
            remote(r2.at[rows], r2.at[rows], rs_ssem, r2_rsem.at[j, p], ep, tp).wait_recv()
            whole = psend[0, rows, :].astype(F32) + r1[0, rows, :].astype(F32) + r2[rows, :].astype(F32)
            first_slot, n = START[j] + p * SIZES[j] // 2, SIZES[j] // 2
            rsend[first_slot : first_slot + n] = whole.astype(BF16).reshape(n, CAP, 512)
            for s in range(first_slot, first_slot + n):
                if s == 0:
                    rret[ep] = rsend[0]
                else:
                    to = target(ORDER[s], -1)
                    remote(rsend.at[s], rret.at[ep], rt_ssem, rt_rsem, to, tp).start()

    def arrived(j):
        for s in range(max(START[j], 1), START[j] + SIZES[j]):
            remote(recv2.at[s], recv2.at[s], dsend, drecv.at[s], ep, tp).wait_recv()

    first.wait_recv()
    later_core = c == 1
    mine, other = msg[0:128, :], pmsg[0:128, :]
    older = jnp.where(later_core, other, mine)
    newer = jnp.where(later_core, mine, other)
    newer_total = jnp.where(later_core, msg[128:136, :], pmsg[128:136, :])
    joint[...] = column(newer_total) * older + newer
    half = pl.ds(pl.multiple_of(c * 64, 64), 64)
    chmsg[0:64, :] = joint[half, :]
    chmsg[64:72, :] = msg[128:136, :] + pmsg[128:136, :]
    yrecv[y] = chmsg[...]

    def y_share(d):
        return remote(chmsg, yrecv.at[y], ch_ssem, y_rsem.at[d - 1], target((0, d, 0)), tp)

    def z_share(d):
        return remote(zmsg, zrecv.at[d - 1], zm_ssem.at[d - 1], z_rsem.at[d - 1], target((d, 0, 0)), tp)

    for d in range(1, NY):
        y_share(d).start()
    for dc in (0, 1):
        straight((2, 0, dc))
        straight((0, 2, dc))

    for i in range(7, 10):
        loads[i].wait()
    arrived(0)
    expert(0)
    pass_on(NEAR, FAR)
    handed(128, 2)
    handed(128, 3)
    for m in range(1, 4):
        hand_on(flips[m], 0, 128, 4, partner, tp)
    middle(0)
    pass_on(FAR, NEAR)
    pass_on(FAR, FAR)
    for d in NEAR:
        straight((d, 0, 1))
        straight((0, d, 1))
    cols_in = jnp.concatenate(
        [routes_t_ref[...].astype(F32), share_t, jnp.zeros((4, rows2), F32)], axis=0
    )
    unit = (iota((8, 128), 0) == iota((8, 128), 1)).astype(F32)
    cols_out = dot_t0(cols_in, unit, HIGH)
    e_lane = iota((rows2, experts), 1).astype(F32)
    r_cols = [cols_out[:, 0:1], cols_out[:, 1:2]]
    member = ((r_cols[0] == e_lane) | (r_cols[1] == e_lane)).astype(BF16)
    earlier = (iota((rows2, rows2), 0) > iota((rows2, rows2), 1)).astype(BF16)
    rank = dot(earlier, member)
    lanes = iota((rows2, experts * CAP), 1).astype(F32)
    for r in range(2):
        slot = jnp.sum(jnp.where(r_cols[r] == e_lane, rank, 0.0), axis=1, keepdims=True)
        pickm[r] = (lanes == slot + r_cols[r] * CAP).astype(BF16)

    arrived(1)
    expert(1)
    reduce(0)

    def fade_of(row8):
        fade = column(row8)
        return jnp.where(later_core, fade[64:128], fade[0:64])

    for d in range(1, NY):
        y_share(d).wait_recv()
    row_state, row_total = yrecv[0, 0:64, :], yrecv[0, 64:72, :]
    own_state = jnp.zeros_like(row_state)
    own_total = jnp.zeros_like(row_total)
    for k in range(1, NY):
        own_state = jnp.where(y == k, row_state, own_state)
        own_total = jnp.where(y == k, row_total, own_total)
        row_state = fade_of(yrecv[k, 64:72, :]) * row_state + yrecv[k, 0:64, :]
        row_total = row_total + yrecv[k, 64:72, :]
    ymsg[0:64, :], ymsg[64:72, :] = own_state, own_total
    zmsg[0:64, :], zmsg[64:72, :] = row_state, row_total
    for d in range(1, NZ):
        pl.when(z + d < NZ)(z_share(d).start)
    middle(1)
    arrived(2)
    expert(2)
    reduce(1)
    inc[half, :] = jnp.zeros((64, 128), F32)

    def join(k, _):
        cp = remote(zrecv.at[z - k - 1], zrecv.at[z - k - 1], ch_ssem, z_rsem.at[z - k - 1], ep, tp)
        cp.wait_recv()
        fade = fade_of(zrecv[z - k - 1, 64:72, :])
        inc[half, :] = fade * inc[half, :] + zrecv[z - k - 1, 0:64, :]
        return 0

    lax.fori_loop(0, z, join, 0)
    inc[half, :] = fade_of(ymsg[64:72, :]) * inc[half, :] + ymsg[0:64, :]
    second = remote(inc.at[half], inc.at[half], dd_ssem.at[1], dd_rsem.at[1], partner, tp)
    second.start()
    arrived(3)
    expert(3)
    second.wait()
    joined = column(pmsg[128:136, :]) * inc[...] + pmsg[0:128, :]
    entry = jnp.where(later_core, joined, inc[...])
    entry_bd = jnp.concatenate([entry, entry], axis=1) * own_head
    for i in range(att.shape[0] // 128):
        rows = slice(128 * i, 128 * i + 128)
        whole = att[rows, :] + dot(reach[rows, :], entry_bd, HIGH)
        parts = []
        for h in range(2):
            one = whole[:, VALUE_DIM * h : VALUE_DIM * (h + 1)]
            parts.append(one * lax.rsqrt(jnp.mean(one * one, axis=-1, keepdims=True) + EPS))
        out_gate = proj[rows, 512:768]
        rows_out = jnp.concatenate(parts, axis=1) * hgain_ref[...]
        gated[rows, :] = (rows_out * (out_gate * jax.nn.sigmoid(out_gate))).astype(BF16)
    quarter = out1_ref.shape[0]
    mine_cols = pl.ds(pl.multiple_of(tp * 256, 256), 256)
    for m in range(1, 4):
        rows = pl.ds(pl.multiple_of(flips[m] * quarter, quarter), quarter)
        remote(gated.at[rows], spread.at[:, mine_cols], mx_ssem, mx_rsem, ep, flips[m]).start()
    spread[:, mine_cols] = gated[pl.ds(pl.multiple_of(tp * quarter, quarter), quarter), :]

    middle(2)
    arrived(4)
    expert(4)
    reduce(2)
    remote(spread.at[:, 0:768], spread.at[:, 0:768], mx_ssem, mx_rsem, ep, tp).wait_recv()
    handed(384, 4)
    for n in range(4):
        cols = slice(512 * n, 512 * n + 512)
        out1_ref[:, cols] = dot(spread[...], wfull[:, cols]).astype(BF16)
    middle(3)
    middle(4)
    reduce(3)
    reduce(4)

    remote(rret.at[1:experts], rret.at[1:experts], rt_ssem, rt_rsem, ep, tp).wait_recv()
    flat = rret[...].reshape(experts * CAP, 512)
    mixed = jnp.zeros((rows2, 512), F32)
    for r in range(2):
        mixed = mixed + dot(pickm[r], flat) * cols_out[:, 2 + r : 3 + r]
    out2_ref[...] = mixed.astype(BF16)

    remote(send2.at[1:experts], send2.at[1:experts], dsend, drecv.at[0], ep, tp).wait_send()
    remote(relay, relay, dsend, drecv.at[0], ep, tp).wait_send()
    remote(r1, r1, rs_ssem, r1_rsem.at[0, 0], ep, tp).wait_send()
    remote(r2, r2, rs_ssem, r1_rsem.at[0, 0], ep, tp).wait_send()
    for n in (128, 256, 384):
        remote(wfull.at[0:n], wfull.at[0:n], w_ssem, w_rsem.at[0], ep, tp).wait_send()
    remote(spread.at[:, 0:768], spread.at[:, 0:768], mx_ssem, mx_rsem, ep, tp).wait_send()
    remote(rret.at[1:experts], rret.at[1:experts], rt_ssem, rt_rsem, ep, tp).wait_send()
    first.wait_send()
    remote(yrecv.at[0:3], yrecv.at[0:3], ch_ssem, y_rsem.at[0], ep, tp).wait_send()
    for d in range(1, NZ):
        pl.when(z + d < NZ)(z_share(d).wait_send)


def body(
    tokens_first, norm_gain_first, w_query, w_key, w_value, w_outgate, w_decay, decay_bias,
    head_gain, w_mix_out, tokens_second, norm_gain_second, routes, route_logits,
    expert_gate, expert_up, expert_down,
):
    hbm, vmem = pl.BlockSpec(memory_space=pl.ANY), pl.BlockSpec(memory_space=pltpu.VMEM)
    rows1, width = tokens_first.shape
    rows2 = tokens_second.shape[0]
    hidden = expert_gate.shape[2]
    experts = NZ * NY * NC
    quarter = width // 4
    V, D = pltpu.VMEM, pltpu.SemaphoreType.DMA
    return pl.pallas_call(
        kernel,
        out_shape=(
            jax.ShapeDtypeStruct((rows1 // 4, width), BF16),
            jax.ShapeDtypeStruct((rows2, quarter), BF16),
        ),
        in_specs=[
            hbm, vmem, hbm, hbm, hbm, hbm, hbm, vmem, vmem, hbm,
            hbm, vmem, vmem, vmem, hbm, hbm, hbm,
        ],
        out_specs=(vmem, vmem),
        scratch_shapes=[
            V((rows2, width), BF16), V((rows2, width), BF16),
            V((experts, CAP, width), BF16), V((experts, CAP, width), BF16),
            V((18, CAP, width), BF16),
            V((rows1, width), BF16), V((rows1, width), BF16),
            V((width, 896), BF16), V((1024, width), BF16),
            V((width, hidden), BF16), V((width, hidden), BF16), V((hidden, width), BF16),
            V((rows1, 896), F32), V((rows1, 256), F32), V((rows1, 128), F32),
            V((128, 256), F32), V((8, 128), F32), V((136, 128), F32), V((136, 128), F32),
            V((128, 128), F32), V((128, 128), F32),
            V((4, experts * CAP, quarter), BF16), V((2, experts * CAP, quarter), BF16),
            V((experts * CAP, quarter), BF16), V((experts * CAP, quarter), BF16),
            V((experts, CAP, quarter), BF16), V((experts, CAP, quarter), BF16),
            V((rows1, 256), BF16), V((rows1 // 4, 1024), BF16),
            V((2, rows2, experts * CAP), BF16),
            V((max(SIZES) * CAP, hidden), BF16), V((72, 128), F32), V((72, 128), F32),
            V((72, 128), F32), V((NY, 72, 128), F32), V((NZ - 1, 72, 128), F32),
            D((11,)), D(()), D((32,)), D((18,)), D(()), D((CHUNKS, 2)), D((CHUNKS, 2)), D(()), D((5,)),
            D(()), D(()), D(()), D(()),
            D((2,)), D((2,)), D(()), D((3,)), D((3,)), D((3,)),
        ],
        compiler_params=pltpu.CompilerParams(
            collective_id=0, has_side_effects=True, vmem_limit_bytes=63 * 2**20
        ),
        name="layer",
    )(
        tokens_first, norm_gain_first.reshape(1, -1), w_query, w_key, w_value, w_outgate, w_decay,
        decay_bias, head_gain.reshape(1, -1), w_mix_out, tokens_second,
        norm_gain_second.reshape(1, -1), routes.T, route_logits.T,
        expert_gate, expert_up, expert_down,
    )


def solution(mesh):
    ep_tp = ("ep", "tp")
    in_specs = (
        P("ep", None), P(), P(None, "tp"), P(None, "tp"), P(None, "tp"), P(None, "tp"),
        P(None, "tp"), P("ep", "tp"), P("tp"), P("tp", None), P("ep", None), P(), P("ep", None),
        P("ep", None), P("ep", None, "tp"), P("ep", None, "tp"), P("ep", "tp", None),
    )
    out_specs = (P(ep_tp, None), P("ep", "tp"))
    return jax.shard_map(body, mesh=mesh, in_specs=in_specs, out_specs=out_specs, check_vma=False)
```

```python
import jax
import jax.numpy as jnp
from jax import lax
from jax.experimental import pallas as pl
from jax.experimental.pallas import tpu as pltpu
from jax.sharding import PartitionSpec as P

KEY_DIM = 64
VALUE_DIM = 128
BLOCK = 64
CAP = 32
EPS = 1e-06
TEMPER = 16.0
NZ, NY, NC = 4, 4, 2
MESH = pl.DeviceIdType.MESH
HIGH = lax.Precision.HIGHEST
F32, BF16 = jnp.float32, jnp.bfloat16

NEAR, FAR = (1, 3), (2,)
ORDER = (
    [(0, 0, 0), (0, 0, 1)]
    + [o for d in NEAR for o in ((d, 0, 0), (0, d, 0))]
    + [o for c in (0, 1) for o in ((2, 0, c), (0, 2, c))]
    + [o for d in NEAR for o in ((d, 0, 1), (0, d, 1))]
    + [(2, 2, 0), (2, 2, 1)]
    + [o for d in NEAR for o in ((2, d, 0), (d, 2, 1))]
    + [o for d in NEAR for o in ((d, 2, 0), (2, d, 1))]
    + [(dz, dy, c) for c in (0, 1) for dz in NEAR for dy in NEAR]
)
SLOT = {o: s for s, o in enumerate(ORDER)}
SIZES = (6, 8, 6, 4, 4, 4)
START = [sum(SIZES[:j]) for j in range(len(SIZES))]
CHUNKS = len(SIZES)


def dot(a, b, precision=None):
    return jnp.dot(a, b, preferred_element_type=F32, precision=precision)


def dot_t0(a, b, precision=None):
    return lax.dot_general(
        a, b, (((0,), (0,)), ((), ())), preferred_element_type=F32, precision=precision
    )


def dot_t1(a, b, precision=None):
    return lax.dot_general(
        a, b, (((1,), (1,)), ((), ())), preferred_element_type=F32, precision=precision
    )


def iota(shape, dim):
    return lax.broadcasted_iota(jnp.int32, shape, dim)


def rms(rows, gain):
    wide = rows.astype(F32)
    return wide * lax.rsqrt(jnp.mean(wide * wide, axis=-1, keepdims=True) + EPS) * gain


def log_sigmoid(x):
    return jnp.minimum(x, 0.0) - jnp.log1p(jnp.exp(-jnp.abs(x)))


def kernel(
    tok1_h, g1_ref, wq_h, wk_h, wv_h, wo_h, wd_h, bias_ref, hgain_ref, wmix_h,
    tok2_h, g2_ref, routes_t_ref, logits_t_ref, wg_h, wu_h, wdn_h,
    out1_ref, out2_ref,
    tok2, norm2, send2, recv2, relay, tok1, norm1, w1, wfull, wg, wu, wdn, proj, att, reach,
    sbd, total, msg, pmsg, inc, joint, psend, r1, s2, r2, rsend, rret, gated, spread, pickm, hid,
    chmsg, ymsg, zmsg, yrecv, zrecv,
    ld, dsend, drecv, hand_sem, rs_ssem, r1_rsem, r2_rsem, w_ssem, w_rsem, mx_ssem, mx_rsem, rt_ssem, rt_rsem,
    dd_ssem, dd_rsem, ch_ssem, y_rsem, zm_ssem, z_rsem,
):
    ep, tp = lax.axis_index("ep"), lax.axis_index("tp")
    z, y, c = ep // (NY * NC), (ep // NC) % NY, ep % NC
    chip = z * NY + y
    flips = (tp, tp + 1 - 2 * (tp % 2), (tp + 2) % 4, 3 - tp)
    partner = ep + 1 - 2 * c

    def target(o, sign=1):
        dz, dy, dc = o
        return (
            ((z + sign * dz + NZ) % NZ) * (NY * NC)
            + ((y + sign * dy + NY) % NY) * NC
            + (c + dc) % NC
        )

    def remote(src, dst, ssem, rsem, to_ep, to_tp):
        return pltpu.make_async_remote_copy(
            src_ref=src, dst_ref=dst, send_sem=ssem, recv_sem=rsem,
            device_id=(to_ep, to_tp), device_id_type=MESH,
        )

    loads = [
        (tok2_h, tok2), (tok1_h, tok1),
        (wq_h, w1.at[:, 0:128]), (wk_h, w1.at[:, 128:256]), (wv_h, w1.at[:, 256:512]),
        (wo_h, w1.at[:, 512:768]), (wd_h, w1.at[:, 768:896]),
        (wg_h.at[0], wg), (wu_h.at[0], wu), (wdn_h.at[0], wdn),
        (wmix_h, wfull.at[pl.ds(pl.multiple_of(tp * 256, 256), 256)]),
    ]
    loads = [pltpu.make_async_copy(s, d, ld.at[i]) for i, (s, d) in enumerate(loads)]

    barrier = pltpu.get_barrier_semaphore()
    near = [o for o in ORDER[1:] if not (o[0] and o[1])]
    for o in near:
        pl.semaphore_signal(barrier, inc=1, device_id=(target(o), tp), device_id_type=MESH)
    for m in (1, 3):
        pl.semaphore_signal(barrier, inc=1, device_id=(ep, flips[m]), device_id_type=MESH)

    for cp in loads:
        cp.start()

    rows2 = norm2.shape[0]
    experts = send2.shape[0]
    r0t, r1t = routes_t_ref[0:1, :], routes_t_ref[1:2, :]
    e_sub = iota((experts, rows2), 0)
    gap = logits_t_ref[0:1, :] - logits_t_ref[1:2, :]
    share_t = jnp.concatenate([jax.nn.sigmoid(gap), jax.nn.sigmoid(-gap)], axis=0)
    member_t = ((r0t == e_sub) | (r1t == e_sub)).astype(F32)
    before_t = (iota((rows2, rows2), 0) < iota((rows2, rows2), 1)).astype(BF16)
    rank_t = dot(member_t.astype(BF16), before_t)
    place_t = jnp.where(member_t > 0.0, rank_t, -1.0)
    loads[0].wait()
    norm2[...] = rms(tok2[...], g2_ref[...]).astype(BF16)
    for g in range(experts // 8):
        place = place_t[8 * g : 8 * g + 8]
        want = iota((8, CAP, rows2), 1).astype(F32)
        pick = (place[:, None, :] == want).astype(BF16).reshape(8 * CAP, rows2)
        for n in range(norm2.shape[1] // 512):
            cols = slice(512 * n, 512 * n + 512)
            send2[8 * g : 8 * g + 8, :, cols] = (
                dot(pick, norm2[:, cols]).astype(BF16).reshape(8, CAP, 512)
            )
    pl.semaphore_wait(barrier, len(near) + 2)

    def straight(o):
        to, s = target(o), SLOT[o]
        remote(send2.at[to], recv2.at[s], dsend, drecv.at[s], to, tp).start()

    def turn(o):
        dz, dy, dc = o
        corner = target((0, dy, 1) if dc else (dz, 0, 0))
        onward = target((dz, 0, 0) if dc else (0, dy, 0))
        k = (dc * 3 + dz - 1) * 3 + dy - 1
        into = remote(send2.at[target(o)], relay.at[k], dsend, hand_sem.at[k], corner, tp)
        s = SLOT[o]
        out = remote(relay.at[k], recv2.at[s], dsend, drecv.at[s], onward, tp)
        return into, out

    def leave(dzs, dys):
        for dz in dzs:
            for dy in dys:
                turn((dz, dy, 0))[0].start()
                turn((dy, dz, 1))[0].start()

    def pass_on(dzs, dys):
        for dz in dzs:
            for dy in dys:
                for o in ((dz, dy, 0), (dy, dz, 1)):
                    into, out = turn(o)
                    into.wait_recv()
                    out.start()

    straight((0, 0, 1))
    for d in NEAR:
        straight((d, 0, 0))
        straight((0, d, 0))
    leave(FAR, FAR)
    leave(FAR, NEAR)
    for dc in (0, 1):
        straight((2, 0, dc))
        straight((0, 2, dc))
    leave(NEAR, FAR)

    def shard_rows(t, core, lo, n):
        start = t * 256 + core * 128 + lo
        return pl.ds(pl.multiple_of(start, 64), n)

    def hand_on(owner, lo, n, k, to_ep, to_tp):
        rows = shard_rows(owner, c, lo, n)
        remote(wfull.at[rows], wfull.at[rows], w_ssem, w_rsem.at[k], to_ep, to_tp).start()

    def handed(n, k):
        remote(wfull.at[0:n], wfull.at[0:n], w_ssem, w_rsem.at[k], ep, tp).wait_recv()

    loads[10].wait()
    hand_on(tp, 0, 64, 0, ep, flips[1])
    hand_on(tp, 64, 64, 1, ep, flips[3])
    recv2[0] = send2[ep]

    loads[1].wait()
    for i in range(tok1.shape[0] // 128):
        rows = slice(128 * i, 128 * i + 128)
        norm1[rows, :] = rms(tok1[rows, :], g1_ref[...]).astype(BF16)
    for i in range(2, 7):
        loads[i].wait()
    for lo, hi in ((0, 256), (256, 512), (512, 768), (768, 896)):
        proj[:, lo:hi] = dot(norm1[...], w1[:, lo:hi])
    sbd[...] = jnp.zeros_like(sbd)
    total[...] = jnp.zeros_like(total)
    own_head = (iota(sbd.shape, 0) // KEY_DIM == iota(sbd.shape, 1) // VALUE_DIM).astype(F32)
    tri = (iota((BLOCK, BLOCK), 0) >= iota((BLOCK, BLOCK), 1)).astype(F32)
    head_lane = iota((BLOCK, 2 * KEY_DIM), 1) // KEY_DIM

    def block(b, _):
        rows = pl.ds(pl.multiple_of(b * BLOCK, BLOCK), BLOCK)
        query = (proj[rows, 0:128] * KEY_DIM ** (-0.5)).astype(BF16).astype(F32)
        key = proj[rows, 128:256].astype(BF16).astype(F32)
        value = proj[rows, 256:512].astype(BF16).astype(F32)
        log_decay = log_sigmoid(proj[rows, 768:896] + bias_ref[pl.ds(b, 1), :]) / TEMPER
        cumul = dot(tri, log_decay, HIGH)
        final = cumul[BLOCK - 1 : BLOCK, :]
        forward = query * jnp.exp(cumul)
        behind = key * jnp.exp(-cumul)
        fading = key * jnp.exp(final - cumul)
        within = []
        for h in range(2):
            mine = jnp.where(head_lane == h, forward, 0.0)
            scores = dot_t1(mine, behind, HIGH)
            scores = jnp.where(tri > 0.0, scores, 0.0)
            within.append(dot(scores, value[:, VALUE_DIM * h : VALUE_DIM * (h + 1)], HIGH))
        att[rows, :] = jnp.concatenate(within, axis=1) + dot(forward, sbd[...], HIGH)
        fall = dot_t0(log_decay, jnp.ones((BLOCK, sbd.shape[1]), F32), HIGH)
        sbd[...] = jnp.exp(fall) * sbd[...] + own_head * dot_t0(fading, value, HIGH)
        reach[rows, :] = query * jnp.exp(cumul + total[0:1, :])
        total[0:1, :] = total[0:1, :] + final
        return 0

    blocks = proj.shape[0] // BLOCK
    lax.fori_loop(0, blocks // 2, block, 0)
    handed(64, 0)
    hand_on(tp, 0, 64, 2, ep, flips[3])
    hand_on(flips[1], 0, 64, 2, ep, flips[3])
    handed(64, 1)
    hand_on(tp, 64, 64, 3, ep, flips[1])
    hand_on(flips[3], 64, 64, 3, ep, flips[1])
    lax.fori_loop(blocks // 2, blocks, block, 0)
    msg[0:64, :] = sbd[0:64, 0:128]
    msg[64:128, :] = sbd[64:128, 128:256]
    msg[128:136, :] = total[...]
    first = remote(msg, pmsg, dd_ssem.at[0], dd_rsem.at[0], partner, tp)
    first.start()

    def column(row8):
        return jnp.exp(dot_t0(row8, jnp.ones((8, 128), F32), HIGH))

    def rows_of(j, p=None):
        lo, n = START[j] * CAP, SIZES[j] * CAP
        return slice(lo, lo + n) if p is None else slice(lo + p * n // 2, lo + (p + 1) * n // 2)

    def expert(j):
        n = SIZES[j]
        x_rows = recv2[START[j] : START[j] + n].reshape(n * CAP, recv2.shape[2])
        for lo in range(0, hid.shape[1], 256):
            cols = slice(lo, lo + 256)
            gate = dot(x_rows, wg[:, cols])
            up = dot(x_rows, wu[:, cols])
            hid[0 : n * CAP, cols] = (gate * jax.nn.sigmoid(gate) * up).astype(BF16)
        for m in (2, 1, 3, 0):
            cols = pl.ds(pl.multiple_of(flips[m] * 512, 512), 512)
            psend[m, rows_of(j), :] = dot(hid[0 : n * CAP, :], wdn[:, cols]).astype(BF16)
            for p, q, k in ((0, 1, 0), (0, 2, 1), (1, 3, 0), (1, 2, 1)):
                if q == m:
                    remote(
                        psend.at[m, rows_of(j, p)], r1.at[k, rows_of(j, p)],
                        rs_ssem, r1_rsem.at[j, p], ep, flips[1 + 2 * p],
                    ).start()

    def middle(j):
        for p in range(2):
            rows = rows_of(j, p)
            both = r1.at[:, rows]
            remote(both, both, rs_ssem, r1_rsem.at[j, p], ep, tp).wait_recv()
            pair = psend[3 - 2 * p, rows, :].astype(F32) + r1[1, rows, :].astype(F32)
            s2[rows, :] = pair.astype(BF16)
            remote(s2.at[rows], r2.at[rows], rs_ssem, r2_rsem.at[j, p], ep, flips[3 - 2 * p]).start()

    def reduce(j):
        for p in range(2):
            rows = rows_of(j, p)
            remote(r2.at[rows], r2.at[rows], rs_ssem, r2_rsem.at[j, p], ep, tp).wait_recv()
            whole = psend[0, rows, :].astype(F32) + r1[0, rows, :].astype(F32) + r2[rows, :].astype(F32)
            first_slot, n = START[j] + p * SIZES[j] // 2, SIZES[j] // 2
            rsend[first_slot : first_slot + n] = whole.astype(BF16).reshape(n, CAP, 512)
            for s in range(first_slot, first_slot + n):
                if s == 0:
                    rret[ep] = rsend[0]
                else:
                    to = target(ORDER[s], -1)
                    remote(rsend.at[s], rret.at[ep], rt_ssem, rt_rsem, to, tp).start()

    def arrived(j):
        for s in range(max(START[j], 1), START[j] + SIZES[j]):
            remote(recv2.at[s], recv2.at[s], dsend, drecv.at[s], ep, tp).wait_recv()

    first.wait_recv()
    later_core = c == 1
    mine, other = msg[0:128, :], pmsg[0:128, :]
    older = jnp.where(later_core, other, mine)
    newer = jnp.where(later_core, mine, other)
    newer_total = jnp.where(later_core, msg[128:136, :], pmsg[128:136, :])
    joint[...] = column(newer_total) * older + newer
    half = pl.ds(pl.multiple_of(c * 64, 64), 64)
    chmsg[0:64, :] = joint[half, :]
    chmsg[64:72, :] = msg[128:136, :] + pmsg[128:136, :]
    yrecv[y] = chmsg[...]

    def y_share(d):
        return remote(chmsg, yrecv.at[y], ch_ssem, y_rsem.at[d - 1], target((0, d, 0)), tp)

    def z_share(d):
        return remote(zmsg, zrecv.at[d - 1], zm_ssem.at[d - 1], z_rsem.at[d - 1], target((d, 0, 0)), tp)

    for d in range(1, NY):
        y_share(d).start()

    for d in NEAR:
        straight((d, 0, 1))
        straight((0, d, 1))
    leave(NEAR, NEAR)
    for i in range(7, 10):
        loads[i].wait()
    arrived(0)
    expert(0)
    pass_on(FAR, FAR)
    pass_on(FAR, NEAR)
    pass_on(NEAR, FAR)
    handed(128, 2)
    handed(128, 3)
    for m in range(1, 4):
        hand_on(flips[m], 0, 128, 4, partner, tp)
    arrived(1)
    expert(1)
    middle(0)
    def fade_of(row8):
        fade = column(row8)
        return jnp.where(later_core, fade[64:128], fade[0:64])

    for d in range(1, NY):
        y_share(d).wait_recv()
    row_state, row_total = yrecv[0, 0:64, :], yrecv[0, 64:72, :]
    own_state = jnp.zeros_like(row_state)
    own_total = jnp.zeros_like(row_total)
    for k in range(1, NY):
        own_state = jnp.where(y == k, row_state, own_state)
        own_total = jnp.where(y == k, row_total, own_total)
        row_state = fade_of(yrecv[k, 64:72, :]) * row_state + yrecv[k, 0:64, :]
        row_total = row_total + yrecv[k, 64:72, :]
    ymsg[0:64, :], ymsg[64:72, :] = own_state, own_total
    zmsg[0:64, :], zmsg[64:72, :] = row_state, row_total
    for d in range(1, NZ):
        pl.when(z + d < NZ)(z_share(d).start)
    pass_on(NEAR, NEAR)
    cols_in = jnp.concatenate(
        [routes_t_ref[...].astype(F32), share_t, jnp.zeros((4, rows2), F32)], axis=0
    )
    unit = (iota((8, 128), 0) == iota((8, 128), 1)).astype(F32)
    cols_out = dot_t0(cols_in, unit, HIGH)
    e_lane = iota((rows2, experts), 1).astype(F32)
    r_cols = [cols_out[:, 0:1], cols_out[:, 1:2]]
    member = ((r_cols[0] == e_lane) | (r_cols[1] == e_lane)).astype(BF16)
    earlier = (iota((rows2, rows2), 0) > iota((rows2, rows2), 1)).astype(BF16)
    rank = dot(earlier, member)
    lanes = iota((rows2, experts * CAP), 1).astype(F32)
    for r in range(2):
        slot = jnp.sum(jnp.where(r_cols[r] == e_lane, rank, 0.0), axis=1, keepdims=True)
        pickm[r] = (lanes == slot + r_cols[r] * CAP).astype(BF16)

    reduce(0)
    middle(1)
    arrived(2)
    expert(2)
    reduce(1)
    arrived(3)
    expert(3)
    inc[half, :] = jnp.zeros((64, 128), F32)

    def join(k, _):
        cp = remote(zrecv.at[z - k - 1], zrecv.at[z - k - 1], ch_ssem, z_rsem.at[z - k - 1], ep, tp)
        cp.wait_recv()
        fade = fade_of(zrecv[z - k - 1, 64:72, :])
        inc[half, :] = fade * inc[half, :] + zrecv[z - k - 1, 0:64, :]
        return 0

    lax.fori_loop(0, z, join, 0)
    inc[half, :] = fade_of(ymsg[64:72, :]) * inc[half, :] + ymsg[0:64, :]
    second = remote(inc.at[half], inc.at[half], dd_ssem.at[1], dd_rsem.at[1], partner, tp)
    second.start()
    middle(2)
    arrived(4)
    expert(4)
    second.wait()
    joined = column(pmsg[128:136, :]) * inc[...] + pmsg[0:128, :]
    entry = jnp.where(later_core, joined, inc[...])
    entry_bd = jnp.concatenate([entry, entry], axis=1) * own_head
    for i in range(att.shape[0] // 128):
        rows = slice(128 * i, 128 * i + 128)
        whole = att[rows, :] + dot(reach[rows, :], entry_bd, HIGH)
        parts = []
        for h in range(2):
            one = whole[:, VALUE_DIM * h : VALUE_DIM * (h + 1)]
            parts.append(one * lax.rsqrt(jnp.mean(one * one, axis=-1, keepdims=True) + EPS))
        out_gate = proj[rows, 512:768]
        rows_out = jnp.concatenate(parts, axis=1) * hgain_ref[...]
        gated[rows, :] = (rows_out * (out_gate * jax.nn.sigmoid(out_gate))).astype(BF16)
    quarter = out1_ref.shape[0]
    mine_cols = pl.ds(pl.multiple_of(tp * 256, 256), 256)
    for m in range(1, 4):
        rows = pl.ds(pl.multiple_of(flips[m] * quarter, quarter), quarter)
        remote(gated.at[rows], spread.at[:, mine_cols], mx_ssem, mx_rsem, ep, flips[m]).start()
    spread[:, mine_cols] = gated[pl.ds(pl.multiple_of(tp * quarter, quarter), quarter), :]

    arrived(5)
    expert(5)
    middle(3)
    reduce(2)
    middle(4)
    middle(5)
    reduce(3)
    remote(spread.at[:, 0:768], spread.at[:, 0:768], mx_ssem, mx_rsem, ep, tp).wait_recv()
    handed(384, 4)
    for n in range(4):
        cols = slice(512 * n, 512 * n + 512)
        out1_ref[:, cols] = dot(spread[...], wfull[:, cols]).astype(BF16)
    reduce(4)
    reduce(5)

    remote(rret.at[1:experts], rret.at[1:experts], rt_ssem, rt_rsem, ep, tp).wait_recv()
    flat = rret[...].reshape(experts * CAP, 512)
    mixed = jnp.zeros((rows2, 512), F32)
    for r in range(2):
        mixed = mixed + dot(pickm[r], flat) * cols_out[:, 2 + r : 3 + r]
    out2_ref[...] = mixed.astype(BF16)

    remote(send2.at[1:experts], send2.at[1:experts], dsend, drecv.at[0], ep, tp).wait_send()
    remote(relay, relay, dsend, drecv.at[0], ep, tp).wait_send()
    remote(r1, r1, rs_ssem, r1_rsem.at[0, 0], ep, tp).wait_send()
    remote(r2, r2, rs_ssem, r1_rsem.at[0, 0], ep, tp).wait_send()
    for n in (128, 256, 384):
        remote(wfull.at[0:n], wfull.at[0:n], w_ssem, w_rsem.at[0], ep, tp).wait_send()
    remote(spread.at[:, 0:768], spread.at[:, 0:768], mx_ssem, mx_rsem, ep, tp).wait_send()
    remote(rret.at[1:experts], rret.at[1:experts], rt_ssem, rt_rsem, ep, tp).wait_send()
    first.wait_send()
    remote(yrecv.at[0:3], yrecv.at[0:3], ch_ssem, y_rsem.at[0], ep, tp).wait_send()
    for d in range(1, NZ):
        pl.when(z + d < NZ)(z_share(d).wait_send)


def body(
    tokens_first, norm_gain_first, w_query, w_key, w_value, w_outgate, w_decay, decay_bias,
    head_gain, w_mix_out, tokens_second, norm_gain_second, routes, route_logits,
    expert_gate, expert_up, expert_down,
):
    hbm, vmem = pl.BlockSpec(memory_space=pl.ANY), pl.BlockSpec(memory_space=pltpu.VMEM)
    rows1, width = tokens_first.shape
    rows2 = tokens_second.shape[0]
    hidden = expert_gate.shape[2]
    experts = NZ * NY * NC
    quarter = width // 4
    V, D = pltpu.VMEM, pltpu.SemaphoreType.DMA
    return pl.pallas_call(
        kernel,
        out_shape=(
            jax.ShapeDtypeStruct((rows1 // 4, width), BF16),
            jax.ShapeDtypeStruct((rows2, quarter), BF16),
        ),
        in_specs=[
            hbm, vmem, hbm, hbm, hbm, hbm, hbm, vmem, vmem, hbm,
            hbm, vmem, vmem, vmem, hbm, hbm, hbm,
        ],
        out_specs=(vmem, vmem),
        scratch_shapes=[
            V((rows2, width), BF16), V((rows2, width), BF16),
            V((experts, CAP, width), BF16), V((experts, CAP, width), BF16),
            V((18, CAP, width), BF16),
            V((rows1, width), BF16), V((rows1, width), BF16),
            V((width, 896), BF16), V((1024, width), BF16),
            V((width, hidden), BF16), V((width, hidden), BF16), V((hidden, width), BF16),
            V((rows1, 896), F32), V((rows1, 256), F32), V((rows1, 128), F32),
            V((128, 256), F32), V((8, 128), F32), V((136, 128), F32), V((136, 128), F32),
            V((128, 128), F32), V((128, 128), F32),
            V((4, experts * CAP, quarter), BF16), V((2, experts * CAP, quarter), BF16),
            V((experts * CAP, quarter), BF16), V((experts * CAP, quarter), BF16),
            V((experts, CAP, quarter), BF16), V((experts, CAP, quarter), BF16),
            V((rows1, 256), BF16), V((rows1 // 4, 1024), BF16),
            V((2, rows2, experts * CAP), BF16),
            V((max(SIZES) * CAP, hidden), BF16), V((72, 128), F32), V((72, 128), F32),
            V((72, 128), F32), V((NY, 72, 128), F32), V((NZ - 1, 72, 128), F32),
            D((11,)), D(()), D((32,)), D((18,)), D(()), D((CHUNKS, 2)), D((CHUNKS, 2)), D(()), D((5,)),
            D(()), D(()), D(()), D(()),
            D((2,)), D((2,)), D(()), D((3,)), D((3,)), D((3,)),
        ],
        compiler_params=pltpu.CompilerParams(
            collective_id=0, has_side_effects=True, vmem_limit_bytes=63 * 2**20
        ),
        name="layer",
    )(
        tokens_first, norm_gain_first.reshape(1, -1), w_query, w_key, w_value, w_outgate, w_decay,
        decay_bias, head_gain.reshape(1, -1), w_mix_out, tokens_second,
        norm_gain_second.reshape(1, -1), routes.T, route_logits.T,
        expert_gate, expert_up, expert_down,
    )


def solution(mesh):
    ep_tp = ("ep", "tp")
    in_specs = (
        P("ep", None), P(), P(None, "tp"), P(None, "tp"), P(None, "tp"), P(None, "tp"),
        P(None, "tp"), P("ep", "tp"), P("tp"), P("tp", None), P("ep", None), P(), P("ep", None),
        P("ep", None), P("ep", None, "tp"), P("ep", None, "tp"), P("ep", "tp", None),
    )
    out_specs = (P(ep_tp, None), P("ep", "tp"))
    return jax.shard_map(body, mesh=mesh, in_specs=in_specs, out_specs=out_specs, check_vma=False)
```

```python
import jax
import jax.numpy as jnp
from jax import lax
from jax.experimental import pallas as pl
from jax.experimental.pallas import tpu as pltpu
from jax.sharding import PartitionSpec as P

KEY_DIM = 64
VALUE_DIM = 128
BLOCK = 64
CAP = 32
EPS = 1e-06
TEMPER = 16.0
NZ, NY, NC = 4, 4, 2
MESH = pl.DeviceIdType.MESH
HIGH = lax.Precision.HIGHEST
F32, BF16 = jnp.float32, jnp.bfloat16

NEAR, FAR = (1, 3), (2,)
ORDER = (
    [(0, 0, 0), (0, 0, 1)]
    + [o for d in NEAR for o in ((d, 0, 0), (0, d, 0))]
    + [o for c in (0, 1) for o in ((2, 0, c), (0, 2, c))]
    + [o for d in NEAR for o in ((d, 0, 1), (0, d, 1))]
    + [(2, 2, 0), (2, 2, 1)]
    + [o for d in NEAR for o in ((2, d, 0), (d, 2, 1))]
    + [o for d in NEAR for o in ((d, 2, 0), (2, d, 1))]
    + [(dz, dy, c) for c in (0, 1) for dz in NEAR for dy in NEAR]
)
SLOT = {o: s for s, o in enumerate(ORDER)}
SIZES = (6, 8, 6, 4, 4, 4)
START = [sum(SIZES[:j]) for j in range(len(SIZES))]
CHUNKS = len(SIZES)


def dot(a, b, precision=None):
    return jnp.dot(a, b, preferred_element_type=F32, precision=precision)


def dot_t0(a, b, precision=None):
    return lax.dot_general(
        a, b, (((0,), (0,)), ((), ())), preferred_element_type=F32, precision=precision
    )


def dot_t1(a, b, precision=None):
    return lax.dot_general(
        a, b, (((1,), (1,)), ((), ())), preferred_element_type=F32, precision=precision
    )


def iota(shape, dim):
    return lax.broadcasted_iota(jnp.int32, shape, dim)


def rms(rows, gain):
    wide = rows.astype(F32)
    return wide * lax.rsqrt(jnp.mean(wide * wide, axis=-1, keepdims=True) + EPS) * gain


def log_sigmoid(x):
    return jnp.minimum(x, 0.0) - jnp.log1p(jnp.exp(-jnp.abs(x)))


def kernel(
    tok1_h, g1_ref, wq_h, wk_h, wv_h, wo_h, wd_h, bias_ref, hgain_ref, wmix_h,
    tok2_h, g2_ref, routes_t_ref, logits_t_ref, wg_h, wu_h, wdn_h,
    out1_ref, out2_ref,
    tok2, norm2, send2, recv2, relay, tok1, norm1, w1, wfull, wg, wu, wdn, proj, att, reach,
    sbd, total, msg, pmsg, inc, joint, psend, r1, s2, r2, rsend, rret, gated, spread, pickm, hid,
    chmsg, ymsg, zmsg, yrecv, zrecv,
    ld, dsend, drecv, hand_sem, rs_ssem, r1_rsem, r2_rsem, w_ssem, w_rsem, mx_ssem, mx_rsem, rt_ssem, rt_rsem,
    dd_ssem, dd_rsem, ch_ssem, y_rsem, zm_ssem, z_rsem,
):
    ep, tp = lax.axis_index("ep"), lax.axis_index("tp")
    z, y, c = ep // (NY * NC), (ep // NC) % NY, ep % NC
    chip = z * NY + y
    flips = (tp, tp + 1 - 2 * (tp % 2), (tp + 2) % 4, 3 - tp)
    partner = ep + 1 - 2 * c

    def target(o, sign=1):
        dz, dy, dc = o
        return (
            ((z + sign * dz + NZ) % NZ) * (NY * NC)
            + ((y + sign * dy + NY) % NY) * NC
            + (c + dc) % NC
        )

    def remote(src, dst, ssem, rsem, to_ep, to_tp):
        return pltpu.make_async_remote_copy(
            src_ref=src, dst_ref=dst, send_sem=ssem, recv_sem=rsem,
            device_id=(to_ep, to_tp), device_id_type=MESH,
        )

    loads = [
        (tok2_h, tok2), (tok1_h, tok1),
        (wq_h, w1.at[:, 0:128]), (wk_h, w1.at[:, 128:256]), (wv_h, w1.at[:, 256:512]),
        (wo_h, w1.at[:, 512:768]), (wd_h, w1.at[:, 768:896]),
        (wg_h.at[0], wg), (wu_h.at[0], wu), (wdn_h.at[0], wdn),
        (wmix_h, wfull.at[pl.ds(pl.multiple_of(tp * 256, 256), 256)]),
    ]
    loads = [pltpu.make_async_copy(s, d, ld.at[i]) for i, (s, d) in enumerate(loads)]

    barrier = pltpu.get_barrier_semaphore()
    near = [o for o in ORDER[1:] if not (o[0] and o[1])]
    for o in near:
        pl.semaphore_signal(barrier, inc=1, device_id=(target(o), tp), device_id_type=MESH)
    for m in (1, 3):
        pl.semaphore_signal(barrier, inc=1, device_id=(ep, flips[m]), device_id_type=MESH)

    for i in (0, 10, 1, 2, 3, 4, 5, 6):
        loads[i].start()

    rows2 = norm2.shape[0]
    experts = send2.shape[0]
    r0t, r1t = routes_t_ref[0:1, :], routes_t_ref[1:2, :]
    e_sub = iota((experts, rows2), 0)
    gap = logits_t_ref[0:1, :] - logits_t_ref[1:2, :]
    share_t = jnp.concatenate([jax.nn.sigmoid(gap), jax.nn.sigmoid(-gap)], axis=0)
    member_t = ((r0t == e_sub) | (r1t == e_sub)).astype(F32)
    before_t = (iota((rows2, rows2), 0) < iota((rows2, rows2), 1)).astype(BF16)
    rank_t = dot(member_t.astype(BF16), before_t)
    place_t = jnp.where(member_t > 0.0, rank_t, -1.0)
    loads[0].wait()
    norm2[...] = rms(tok2[...], g2_ref[...]).astype(BF16)
    for g in range(experts // 8):
        place = place_t[8 * g : 8 * g + 8]
        want = iota((8, CAP, rows2), 1).astype(F32)
        pick = (place[:, None, :] == want).astype(BF16).reshape(8 * CAP, rows2)
        for n in range(norm2.shape[1] // 512):
            cols = slice(512 * n, 512 * n + 512)
            send2[8 * g : 8 * g + 8, :, cols] = (
                dot(pick, norm2[:, cols]).astype(BF16).reshape(8, CAP, 512)
            )
    pl.semaphore_wait(barrier, len(near) + 2)

    def straight(o):
        to, s = target(o), SLOT[o]
        remote(send2.at[to], recv2.at[s], dsend, drecv.at[s], to, tp).start()

    def turn(o):
        dz, dy, dc = o
        corner = target((0, dy, 1) if dc else (dz, 0, 0))
        onward = target((dz, 0, 0) if dc else (0, dy, 0))
        k = (dc * 3 + dz - 1) * 3 + dy - 1
        into = remote(send2.at[target(o)], relay.at[k], dsend, hand_sem.at[k], corner, tp)
        s = SLOT[o]
        out = remote(relay.at[k], recv2.at[s], dsend, drecv.at[s], onward, tp)
        return into, out

    def leave(dzs, dys):
        for dz in dzs:
            for dy in dys:
                turn((dz, dy, 0))[0].start()
                turn((dy, dz, 1))[0].start()

    def pass_on(dzs, dys):
        for dz in dzs:
            for dy in dys:
                for o in ((dz, dy, 0), (dy, dz, 1)):
                    into, out = turn(o)
                    into.wait_recv()
                    out.start()

    straight((0, 0, 1))
    for d in NEAR:
        straight((d, 0, 0))
        straight((0, d, 0))
    leave(FAR, FAR)
    leave(FAR, NEAR)
    for dc in (0, 1):
        straight((2, 0, dc))
        straight((0, 2, dc))
    leave(NEAR, FAR)

    def shard_rows(t, core, lo, n):
        start = t * 256 + core * 128 + lo
        return pl.ds(pl.multiple_of(start, 64), n)

    def hand_on(owner, lo, n, k, to_ep, to_tp):
        rows = shard_rows(owner, c, lo, n)
        remote(wfull.at[rows], wfull.at[rows], w_ssem, w_rsem.at[k], to_ep, to_tp).start()

    def handed(n, k):
        remote(wfull.at[0:n], wfull.at[0:n], w_ssem, w_rsem.at[k], ep, tp).wait_recv()

    for i in range(7, 10):
        loads[i].start()
    loads[10].wait()
    hand_on(tp, 0, 64, 0, ep, flips[1])
    hand_on(tp, 64, 64, 1, ep, flips[3])
    recv2[0] = send2[ep]

    loads[1].wait()
    for i in range(tok1.shape[0] // 128):
        rows = slice(128 * i, 128 * i + 128)
        norm1[rows, :] = rms(tok1[rows, :], g1_ref[...]).astype(BF16)
    for i in range(2, 7):
        loads[i].wait()
    for lo, hi in ((0, 256), (256, 512), (512, 768), (768, 896)):
        proj[:, lo:hi] = dot(norm1[...], w1[:, lo:hi])
    sbd[...] = jnp.zeros_like(sbd)
    total[...] = jnp.zeros_like(total)
    own_head = (iota(sbd.shape, 0) // KEY_DIM == iota(sbd.shape, 1) // VALUE_DIM).astype(F32)
    tri = (iota((BLOCK, BLOCK), 0) >= iota((BLOCK, BLOCK), 1)).astype(F32)
    head_lane = iota((BLOCK, 2 * KEY_DIM), 1) // KEY_DIM

    def block(b, _):
        rows = pl.ds(pl.multiple_of(b * BLOCK, BLOCK), BLOCK)
        query = (proj[rows, 0:128] * KEY_DIM ** (-0.5)).astype(BF16).astype(F32)
        key = proj[rows, 128:256].astype(BF16).astype(F32)
        value = proj[rows, 256:512].astype(BF16).astype(F32)
        log_decay = log_sigmoid(proj[rows, 768:896] + bias_ref[pl.ds(b, 1), :]) / TEMPER
        cumul = dot(tri, log_decay, HIGH)
        final = cumul[BLOCK - 1 : BLOCK, :]
        forward = query * jnp.exp(cumul)
        behind = key * jnp.exp(-cumul)
        fading = key * jnp.exp(final - cumul)
        within = []
        for h in range(2):
            mine = jnp.where(head_lane == h, forward, 0.0)
            scores = dot_t1(mine, behind, HIGH)
            scores = jnp.where(tri > 0.0, scores, 0.0)
            within.append(dot(scores, value[:, VALUE_DIM * h : VALUE_DIM * (h + 1)], HIGH))
        att[rows, :] = jnp.concatenate(within, axis=1) + dot(forward, sbd[...], HIGH)
        fall = dot_t0(log_decay, jnp.ones((BLOCK, sbd.shape[1]), F32), HIGH)
        sbd[...] = jnp.exp(fall) * sbd[...] + own_head * dot_t0(fading, value, HIGH)
        reach[rows, :] = query * jnp.exp(cumul + total[0:1, :])
        total[0:1, :] = total[0:1, :] + final
        return 0

    blocks = proj.shape[0] // BLOCK
    lax.fori_loop(0, blocks // 2, block, 0)
    handed(64, 0)
    hand_on(tp, 0, 64, 2, ep, flips[3])
    hand_on(flips[1], 0, 64, 2, ep, flips[3])
    handed(64, 1)
    hand_on(tp, 64, 64, 3, ep, flips[1])
    hand_on(flips[3], 64, 64, 3, ep, flips[1])
    lax.fori_loop(blocks // 2, blocks, block, 0)
    msg[0:64, :] = sbd[0:64, 0:128]
    msg[64:128, :] = sbd[64:128, 128:256]
    msg[128:136, :] = total[...]
    first = remote(msg, pmsg, dd_ssem.at[0], dd_rsem.at[0], partner, tp)
    first.start()

    def column(row8):
        return jnp.exp(dot_t0(row8, jnp.ones((8, 128), F32), HIGH))

    def rows_of(j, p=None):
        lo, n = START[j] * CAP, SIZES[j] * CAP
        return slice(lo, lo + n) if p is None else slice(lo + p * n // 2, lo + (p + 1) * n // 2)

    def expert(j):
        n = SIZES[j]
        x_rows = recv2[START[j] : START[j] + n].reshape(n * CAP, recv2.shape[2])
        for lo in range(0, hid.shape[1], 256):
            cols = slice(lo, lo + 256)
            gate = dot(x_rows, wg[:, cols])
            up = dot(x_rows, wu[:, cols])
            hid[0 : n * CAP, cols] = (gate * jax.nn.sigmoid(gate) * up).astype(BF16)
        for m in (2, 1, 3, 0):
            cols = pl.ds(pl.multiple_of(flips[m] * 512, 512), 512)
            psend[m, rows_of(j), :] = dot(hid[0 : n * CAP, :], wdn[:, cols]).astype(BF16)
            for p, q, k in ((0, 1, 0), (0, 2, 1), (1, 3, 0), (1, 2, 1)):
                if q == m:
                    remote(
                        psend.at[m, rows_of(j, p)], r1.at[k, rows_of(j, p)],
                        rs_ssem, r1_rsem.at[j, p], ep, flips[1 + 2 * p],
                    ).start()

    def middle(j):
        for p in range(2):
            rows = rows_of(j, p)
            both = r1.at[:, rows]
            remote(both, both, rs_ssem, r1_rsem.at[j, p], ep, tp).wait_recv()
            pair = psend[3 - 2 * p, rows, :].astype(F32) + r1[1, rows, :].astype(F32)
            s2[rows, :] = pair.astype(BF16)
            remote(s2.at[rows], r2.at[rows], rs_ssem, r2_rsem.at[j, p], ep, flips[3 - 2 * p]).start()

    def reduce(j):
        for p in range(2):
            rows = rows_of(j, p)
            remote(r2.at[rows], r2.at[rows], rs_ssem, r2_rsem.at[j, p], ep, tp).wait_recv()
            whole = psend[0, rows, :].astype(F32) + r1[0, rows, :].astype(F32) + r2[rows, :].astype(F32)
            first_slot, n = START[j] + p * SIZES[j] // 2, SIZES[j] // 2
            rsend[first_slot : first_slot + n] = whole.astype(BF16).reshape(n, CAP, 512)
            for s in range(first_slot, first_slot + n):
                if s == 0:
                    rret[ep] = rsend[0]
                else:
                    to = target(ORDER[s], -1)
                    remote(rsend.at[s], rret.at[ep], rt_ssem, rt_rsem, to, tp).start()

    def arrived(j):
        for s in range(max(START[j], 1), START[j] + SIZES[j]):
            remote(recv2.at[s], recv2.at[s], dsend, drecv.at[s], ep, tp).wait_recv()

    first.wait_recv()
    later_core = c == 1
    mine, other = msg[0:128, :], pmsg[0:128, :]
    older = jnp.where(later_core, other, mine)
    newer = jnp.where(later_core, mine, other)
    newer_total = jnp.where(later_core, msg[128:136, :], pmsg[128:136, :])
    joint[...] = column(newer_total) * older + newer
    half = pl.ds(pl.multiple_of(c * 64, 64), 64)
    chmsg[0:64, :] = joint[half, :]
    chmsg[64:72, :] = msg[128:136, :] + pmsg[128:136, :]
    yrecv[y] = chmsg[...]

    def y_share(d):
        return remote(chmsg, yrecv.at[y], ch_ssem, y_rsem.at[d - 1], target((0, d, 0)), tp)

    def z_share(d):
        return remote(zmsg, zrecv.at[d - 1], zm_ssem.at[d - 1], z_rsem.at[d - 1], target((d, 0, 0)), tp)

    for d in range(1, NY):
        y_share(d).start()

    for d in NEAR:
        straight((d, 0, 1))
        straight((0, d, 1))
    leave(NEAR, NEAR)
    for i in range(7, 10):
        loads[i].wait()
    arrived(0)
    expert(0)
    pass_on(FAR, FAR)
    pass_on(FAR, NEAR)
    pass_on(NEAR, FAR)
    handed(128, 2)
    handed(128, 3)
    for m in range(1, 4):
        hand_on(flips[m], 0, 128, 4, partner, tp)
    arrived(1)
    expert(1)
    middle(0)
    def fade_of(row8):
        fade = column(row8)
        return jnp.where(later_core, fade[64:128], fade[0:64])

    for d in range(1, NY):
        y_share(d).wait_recv()
    row_state, row_total = yrecv[0, 0:64, :], yrecv[0, 64:72, :]
    own_state = jnp.zeros_like(row_state)
    own_total = jnp.zeros_like(row_total)
    for k in range(1, NY):
        own_state = jnp.where(y == k, row_state, own_state)
        own_total = jnp.where(y == k, row_total, own_total)
        row_state = fade_of(yrecv[k, 64:72, :]) * row_state + yrecv[k, 0:64, :]
        row_total = row_total + yrecv[k, 64:72, :]
    ymsg[0:64, :], ymsg[64:72, :] = own_state, own_total
    zmsg[0:64, :], zmsg[64:72, :] = row_state, row_total
    for d in range(1, NZ):
        pl.when(z + d < NZ)(z_share(d).start)
    cols_in = jnp.concatenate(
        [routes_t_ref[...].astype(F32), share_t, jnp.zeros((4, rows2), F32)], axis=0
    )
    unit = (iota((8, 128), 0) == iota((8, 128), 1)).astype(F32)
    cols_out = dot_t0(cols_in, unit, HIGH)
    e_lane = iota((rows2, experts), 1).astype(F32)
    r_cols = [cols_out[:, 0:1], cols_out[:, 1:2]]
    member = ((r_cols[0] == e_lane) | (r_cols[1] == e_lane)).astype(BF16)
    earlier = (iota((rows2, rows2), 0) > iota((rows2, rows2), 1)).astype(BF16)
    rank = dot(earlier, member)
    lanes = iota((rows2, experts * CAP), 1).astype(F32)
    for r in range(2):
        slot = jnp.sum(jnp.where(r_cols[r] == e_lane, rank, 0.0), axis=1, keepdims=True)
        pickm[r] = (lanes == slot + r_cols[r] * CAP).astype(BF16)

    pass_on(NEAR, NEAR)
    reduce(0)
    middle(1)
    arrived(2)
    expert(2)
    reduce(1)
    arrived(3)
    expert(3)
    inc[half, :] = jnp.zeros((64, 128), F32)

    def join(k, _):
        cp = remote(zrecv.at[z - k - 1], zrecv.at[z - k - 1], ch_ssem, z_rsem.at[z - k - 1], ep, tp)
        cp.wait_recv()
        fade = fade_of(zrecv[z - k - 1, 64:72, :])
        inc[half, :] = fade * inc[half, :] + zrecv[z - k - 1, 0:64, :]
        return 0

    lax.fori_loop(0, z, join, 0)
    inc[half, :] = fade_of(ymsg[64:72, :]) * inc[half, :] + ymsg[0:64, :]
    second = remote(inc.at[half], inc.at[half], dd_ssem.at[1], dd_rsem.at[1], partner, tp)
    second.start()
    middle(2)
    arrived(4)
    expert(4)
    second.wait()
    joined = column(pmsg[128:136, :]) * inc[...] + pmsg[0:128, :]
    entry = jnp.where(later_core, joined, inc[...])
    entry_bd = jnp.concatenate([entry, entry], axis=1) * own_head
    for i in range(att.shape[0] // 128):
        rows = slice(128 * i, 128 * i + 128)
        whole = att[rows, :] + dot(reach[rows, :], entry_bd, HIGH)
        parts = []
        for h in range(2):
            one = whole[:, VALUE_DIM * h : VALUE_DIM * (h + 1)]
            parts.append(one * lax.rsqrt(jnp.mean(one * one, axis=-1, keepdims=True) + EPS))
        out_gate = proj[rows, 512:768]
        rows_out = jnp.concatenate(parts, axis=1) * hgain_ref[...]
        gated[rows, :] = (rows_out * (out_gate * jax.nn.sigmoid(out_gate))).astype(BF16)
    quarter = out1_ref.shape[0]
    mine_cols = pl.ds(pl.multiple_of(tp * 256, 256), 256)
    spread[:, mine_cols] = gated[pl.ds(pl.multiple_of(tp * quarter, quarter), quarter), :]

    arrived(5)
    expert(5)
    middle(3)
    reduce(2)
    middle(4)
    middle(5)
    for m in range(1, 4):
        rows = pl.ds(pl.multiple_of(flips[m] * quarter, quarter), quarter)
        remote(gated.at[rows], spread.at[:, mine_cols], mx_ssem, mx_rsem, ep, flips[m]).start()
    reduce(3)
    reduce(4)
    reduce(5)
    remote(spread.at[:, 0:768], spread.at[:, 0:768], mx_ssem, mx_rsem, ep, tp).wait_recv()
    handed(384, 4)
    for n in range(4):
        cols = slice(512 * n, 512 * n + 512)
        out1_ref[:, cols] = dot(spread[...], wfull[:, cols]).astype(BF16)

    remote(rret.at[1:experts], rret.at[1:experts], rt_ssem, rt_rsem, ep, tp).wait_recv()
    flat = rret[...].reshape(experts * CAP, 512)
    mixed = jnp.zeros((rows2, 512), F32)
    for r in range(2):
        mixed = mixed + dot(pickm[r], flat) * cols_out[:, 2 + r : 3 + r]
    out2_ref[...] = mixed.astype(BF16)

    remote(send2.at[1:experts], send2.at[1:experts], dsend, drecv.at[0], ep, tp).wait_send()
    remote(relay, relay, dsend, drecv.at[0], ep, tp).wait_send()
    remote(r1, r1, rs_ssem, r1_rsem.at[0, 0], ep, tp).wait_send()
    remote(r2, r2, rs_ssem, r1_rsem.at[0, 0], ep, tp).wait_send()
    for n in (128, 256, 384):
        remote(wfull.at[0:n], wfull.at[0:n], w_ssem, w_rsem.at[0], ep, tp).wait_send()
    remote(spread.at[:, 0:768], spread.at[:, 0:768], mx_ssem, mx_rsem, ep, tp).wait_send()
    remote(rret.at[1:experts], rret.at[1:experts], rt_ssem, rt_rsem, ep, tp).wait_send()
    first.wait_send()
    remote(yrecv.at[0:3], yrecv.at[0:3], ch_ssem, y_rsem.at[0], ep, tp).wait_send()
    for d in range(1, NZ):
        pl.when(z + d < NZ)(z_share(d).wait_send)


def write_out(first_ref, second_ref, out1_ref, out2_ref):
    out1_ref[...] = first_ref[...]
    out2_ref[...] = second_ref[...]


def body(
    tokens_first, norm_gain_first, w_query, w_key, w_value, w_outgate, w_decay, decay_bias,
    head_gain, w_mix_out, tokens_second, norm_gain_second, routes, route_logits,
    expert_gate, expert_up, expert_down,
):
    hbm, vmem = pl.BlockSpec(memory_space=pl.ANY), pl.BlockSpec(memory_space=pltpu.VMEM)
    rows1, width = tokens_first.shape
    rows2 = tokens_second.shape[0]
    hidden = expert_gate.shape[2]
    experts = NZ * NY * NC
    quarter = width // 4
    V, D = pltpu.VMEM, pltpu.SemaphoreType.DMA
    first, second = pl.pallas_call(
        kernel,
        out_shape=(
            jax.ShapeDtypeStruct((rows1 // 4, width), BF16),
            jax.ShapeDtypeStruct((rows2, quarter), BF16),
        ),
        in_specs=[
            hbm, vmem, hbm, hbm, hbm, hbm, hbm, vmem, vmem, hbm,
            hbm, vmem, vmem, vmem, hbm, hbm, hbm,
        ],
        out_specs=(vmem, vmem),
        scratch_shapes=[
            V((rows2, width), BF16), V((rows2, width), BF16),
            V((experts, CAP, width), BF16), V((experts, CAP, width), BF16),
            V((18, CAP, width), BF16),
            V((rows1, width), BF16), V((rows1, width), BF16),
            V((width, 896), BF16), V((1024, width), BF16),
            V((width, hidden), BF16), V((width, hidden), BF16), V((hidden, width), BF16),
            V((rows1, 896), F32), V((rows1, 256), F32), V((rows1, 128), F32),
            V((128, 256), F32), V((8, 128), F32), V((136, 128), F32), V((136, 128), F32),
            V((128, 128), F32), V((128, 128), F32),
            V((4, experts * CAP, quarter), BF16), V((2, experts * CAP, quarter), BF16),
            V((experts * CAP, quarter), BF16), V((experts * CAP, quarter), BF16),
            V((experts, CAP, quarter), BF16), V((experts, CAP, quarter), BF16),
            V((rows1, 256), BF16), V((rows1 // 4, 1024), BF16),
            V((2, rows2, experts * CAP), BF16),
            V((max(SIZES) * CAP, hidden), BF16), V((72, 128), F32), V((72, 128), F32),
            V((72, 128), F32), V((NY, 72, 128), F32), V((NZ - 1, 72, 128), F32),
            D((11,)), D(()), D((32,)), D((18,)), D(()), D((CHUNKS, 2)), D((CHUNKS, 2)), D(()), D((5,)),
            D(()), D(()), D(()), D(()),
            D((2,)), D((2,)), D(()), D((3,)), D((3,)), D((3,)),
        ],
        compiler_params=pltpu.CompilerParams(
            collective_id=0, has_side_effects=True, vmem_limit_bytes=63 * 2**20
        ),
        name="layer",
    )(
        tokens_first, norm_gain_first.reshape(1, -1), w_query, w_key, w_value, w_outgate, w_decay,
        decay_bias, head_gain.reshape(1, -1), w_mix_out, tokens_second,
        norm_gain_second.reshape(1, -1), routes.T, route_logits.T,
        expert_gate, expert_up, expert_down,
    )
    return pl.pallas_call(
        write_out,
        out_shape=(
            jax.ShapeDtypeStruct(first.shape, BF16), jax.ShapeDtypeStruct(second.shape, BF16)
        ),
        in_specs=[vmem, vmem],
        out_specs=(vmem, vmem),
        compiler_params=pltpu.CompilerParams(vmem_limit_bytes=4 * 2**20),
        name="write_out",
    )(first, second)


def solution(mesh):
    ep_tp = ("ep", "tp")
    in_specs = (
        P("ep", None), P(), P(None, "tp"), P(None, "tp"), P(None, "tp"), P(None, "tp"),
        P(None, "tp"), P("ep", "tp"), P("tp"), P("tp", None), P("ep", None), P(), P("ep", None),
        P("ep", None), P("ep", None, "tp"), P("ep", None, "tp"), P("ep", "tp", None),
    )
    out_specs = (P(ep_tp, None), P("ep", "tp"))
    return jax.shard_map(body, mesh=mesh, in_specs=in_specs, out_specs=out_specs, check_vma=False)
```

```python
import jax
import jax.numpy as jnp
from jax import lax
from jax.experimental import pallas as pl
from jax.experimental.pallas import tpu as pltpu
from jax.sharding import PartitionSpec as P

KEY_DIM = 64
VALUE_DIM = 128
BLOCK = 64
CAP = 32
EPS = 1e-06
TEMPER = 16.0
NZ, NY, NC = 4, 4, 2
MESH = pl.DeviceIdType.MESH
HIGH = lax.Precision.HIGHEST
F32, BF16 = jnp.float32, jnp.bfloat16

NEAR, FAR = (1, 3), (2,)
ORDER = (
    [(0, 0, 0), (0, 0, 1)]
    + [o for d in NEAR for o in ((d, 0, 0), (0, d, 0))]
    + [o for c in (0, 1) for o in ((2, 0, c), (0, 2, c))]
    + [o for d in NEAR for o in ((d, 0, 1), (0, d, 1))]
    + [(2, 2, 0), (2, 2, 1)]
    + [o for d in NEAR for o in ((2, d, 0), (d, 2, 1))]
    + [o for d in NEAR for o in ((d, 2, 0), (2, d, 1))]
    + [(dz, dy, c) for c in (0, 1) for dz in NEAR for dy in NEAR]
)
SLOT = {o: s for s, o in enumerate(ORDER)}
SIZES = (6, 8, 6, 4, 4, 4)
START = [sum(SIZES[:j]) for j in range(len(SIZES))]
CHUNKS = len(SIZES)


def dot(a, b, precision=None):
    return jnp.dot(a, b, preferred_element_type=F32, precision=precision)


def dot_t0(a, b, precision=None):
    return lax.dot_general(
        a, b, (((0,), (0,)), ((), ())), preferred_element_type=F32, precision=precision
    )


def dot_t1(a, b, precision=None):
    return lax.dot_general(
        a, b, (((1,), (1,)), ((), ())), preferred_element_type=F32, precision=precision
    )


def iota(shape, dim):
    return lax.broadcasted_iota(jnp.int32, shape, dim)


def rms(rows, gain):
    wide = rows.astype(F32)
    return wide * lax.rsqrt(jnp.mean(wide * wide, axis=-1, keepdims=True) + EPS) * gain


def log_sigmoid(x):
    return jnp.minimum(x, 0.0) - jnp.log1p(jnp.exp(-jnp.abs(x)))


def kernel(
    tok1_h, g1_ref, wq_h, wk_h, wv_h, wo_h, wd_h, bias_ref, hgain_ref, wmix_h,
    tok2_h, g2_ref, routes_t_ref, logits_t_ref, wg_h, wu_h, wdn_h,
    out1_ref, out2_ref,
    tok2, norm2, send2, recv2, relay, tok1, norm1, w1, wfull, wg, wu, wdn, proj, att, reach,
    sbd, total, msg, pmsg, inc, joint, psend, r1, s2, r2, rsend, rret, gated, spread, pickm, hid,
    chmsg, ymsg, zmsg, yrecv, zrecv,
    ld, dsend, drecv, hand_sem, rs_ssem, r1_rsem, r2_rsem, w_ssem, w_rsem, mx_ssem, mx_rsem, rt_ssem, rt_rsem,
    dd_ssem, dd_rsem, ch_ssem, y_rsem, zm_ssem, z_rsem,
):
    ep, tp = lax.axis_index("ep"), lax.axis_index("tp")
    z, y, c = ep // (NY * NC), (ep // NC) % NY, ep % NC
    chip = z * NY + y
    flips = (tp, tp + 1 - 2 * (tp % 2), (tp + 2) % 4, 3 - tp)
    partner = ep + 1 - 2 * c

    def target(o, sign=1):
        dz, dy, dc = o
        return (
            ((z + sign * dz + NZ) % NZ) * (NY * NC)
            + ((y + sign * dy + NY) % NY) * NC
            + (c + dc) % NC
        )

    def remote(src, dst, ssem, rsem, to_ep, to_tp):
        return pltpu.make_async_remote_copy(
            src_ref=src, dst_ref=dst, send_sem=ssem, recv_sem=rsem,
            device_id=(to_ep, to_tp), device_id_type=MESH,
        )

    loads = [
        (tok2_h, tok2), (tok1_h, tok1),
        (wq_h, w1.at[:, 0:128]), (wk_h, w1.at[:, 128:256]), (wv_h, w1.at[:, 256:512]),
        (wo_h, w1.at[:, 512:768]), (wd_h, w1.at[:, 768:896]),
        (wg_h.at[0], wg), (wu_h.at[0], wu), (wdn_h.at[0], wdn),
        (wmix_h, wfull.at[pl.ds(pl.multiple_of(tp * 256, 256), 256)]),
    ]
    loads = [pltpu.make_async_copy(s, d, ld.at[i]) for i, (s, d) in enumerate(loads)]

    barrier = pltpu.get_barrier_semaphore()
    near = [o for o in ORDER[1:] if not (o[0] and o[1])]
    for o in near:
        pl.semaphore_signal(barrier, inc=1, device_id=(target(o), tp), device_id_type=MESH)
    for m in (1, 3):
        pl.semaphore_signal(barrier, inc=1, device_id=(ep, flips[m]), device_id_type=MESH)

    for i in (0, 10, 1, 2, 3, 4, 5, 6):
        loads[i].start()

    rows2 = norm2.shape[0]
    experts = send2.shape[0]
    r0t, r1t = routes_t_ref[0:1, :], routes_t_ref[1:2, :]
    e_sub = iota((experts, rows2), 0)
    gap = logits_t_ref[0:1, :] - logits_t_ref[1:2, :]
    share_t = jnp.concatenate([jax.nn.sigmoid(gap), jax.nn.sigmoid(-gap)], axis=0)
    member_t = ((r0t == e_sub) | (r1t == e_sub)).astype(F32)
    before_t = (iota((rows2, rows2), 0) < iota((rows2, rows2), 1)).astype(BF16)
    rank_t = dot(member_t.astype(BF16), before_t)
    place_t = jnp.where(member_t > 0.0, rank_t, -1.0)
    loads[0].wait()
    norm2[...] = rms(tok2[...], g2_ref[...]).astype(BF16)
    for g in range(experts // 8):
        place = place_t[8 * g : 8 * g + 8]
        want = iota((8, CAP, rows2), 1).astype(F32)
        pick = (place[:, None, :] == want).astype(BF16).reshape(8 * CAP, rows2)
        for n in range(norm2.shape[1] // 512):
            cols = slice(512 * n, 512 * n + 512)
            send2[8 * g : 8 * g + 8, :, cols] = (
                dot(pick, norm2[:, cols]).astype(BF16).reshape(8, CAP, 512)
            )
    pl.semaphore_wait(barrier, len(near) + 2)

    def straight(o):
        to, s = target(o), SLOT[o]
        remote(send2.at[to], recv2.at[s], dsend, drecv.at[s], to, tp).start()

    def turn(o):
        dz, dy, dc = o
        corner = target((0, dy, 1) if dc else (dz, 0, 0))
        onward = target((dz, 0, 0) if dc else (0, dy, 0))
        k = (dc * 3 + dz - 1) * 3 + dy - 1
        into = remote(send2.at[target(o)], relay.at[k], dsend, hand_sem.at[k], corner, tp)
        s = SLOT[o]
        out = remote(relay.at[k], recv2.at[s], dsend, drecv.at[s], onward, tp)
        return into, out

    def leave(dzs, dys):
        for dz in dzs:
            for dy in dys:
                turn((dz, dy, 0))[0].start()
                turn((dy, dz, 1))[0].start()

    def pass_on(dzs, dys):
        for dz in dzs:
            for dy in dys:
                for o in ((dz, dy, 0), (dy, dz, 1)):
                    into, out = turn(o)
                    into.wait_recv()
                    out.start()

    straight((0, 0, 1))
    for d in NEAR:
        straight((d, 0, 0))
        straight((0, d, 0))
    leave(FAR, FAR)
    leave(FAR, NEAR)
    for dc in (0, 1):
        straight((2, 0, dc))
        straight((0, 2, dc))
    leave(NEAR, FAR)

    def shard_rows(t, core, lo, n):
        start = t * 256 + core * 128 + lo
        return pl.ds(pl.multiple_of(start, 64), n)

    def hand_on(owner, lo, n, k, to_ep, to_tp):
        rows = shard_rows(owner, c, lo, n)
        remote(wfull.at[rows], wfull.at[rows], w_ssem, w_rsem.at[k], to_ep, to_tp).start()

    def handed(n, k):
        remote(wfull.at[0:n], wfull.at[0:n], w_ssem, w_rsem.at[k], ep, tp).wait_recv()

    for i in range(7, 10):
        loads[i].start()
    loads[10].wait()
    hand_on(tp, 0, 64, 0, ep, flips[1])
    hand_on(tp, 64, 64, 1, ep, flips[3])
    recv2[0] = send2[ep]

    loads[1].wait()
    for i in range(tok1.shape[0] // 128):
        rows = slice(128 * i, 128 * i + 128)
        norm1[rows, :] = rms(tok1[rows, :], g1_ref[...]).astype(BF16)
    for i in range(2, 7):
        loads[i].wait()
    for lo, hi in ((0, 256), (256, 512), (512, 768), (768, 896)):
        proj[:, lo:hi] = dot(norm1[...], w1[:, lo:hi])
    sbd[...] = jnp.zeros_like(sbd)
    total[...] = jnp.zeros_like(total)
    own_head = (iota(sbd.shape, 0) // KEY_DIM == iota(sbd.shape, 1) // VALUE_DIM).astype(F32)
    tri = (iota((BLOCK, BLOCK), 0) >= iota((BLOCK, BLOCK), 1)).astype(F32)
    head_lane = iota((BLOCK, 2 * KEY_DIM), 1) // KEY_DIM

    def block(b, _):
        rows = pl.ds(pl.multiple_of(b * BLOCK, BLOCK), BLOCK)
        query = (proj[rows, 0:128] * KEY_DIM ** (-0.5)).astype(BF16).astype(F32)
        key = proj[rows, 128:256].astype(BF16).astype(F32)
        value = proj[rows, 256:512].astype(BF16).astype(F32)
        log_decay = log_sigmoid(proj[rows, 768:896] + bias_ref[pl.ds(b, 1), :]) / TEMPER
        cumul = dot(tri, log_decay, HIGH)
        final = cumul[BLOCK - 1 : BLOCK, :]
        forward = query * jnp.exp(cumul)
        behind = key * jnp.exp(-cumul)
        fading = key * jnp.exp(final - cumul)
        within = []
        for h in range(2):
            mine = jnp.where(head_lane == h, forward, 0.0)
            scores = dot_t1(mine, behind, HIGH)
            scores = jnp.where(tri > 0.0, scores, 0.0)
            within.append(dot(scores, value[:, VALUE_DIM * h : VALUE_DIM * (h + 1)], HIGH))
        att[rows, :] = jnp.concatenate(within, axis=1) + dot(forward, sbd[...], HIGH)
        fall = dot_t0(log_decay, jnp.ones((BLOCK, sbd.shape[1]), F32), HIGH)
        sbd[...] = jnp.exp(fall) * sbd[...] + own_head * dot_t0(fading, value, HIGH)
        reach[rows, :] = query * jnp.exp(cumul + total[0:1, :])
        total[0:1, :] = total[0:1, :] + final
        return 0

    blocks = proj.shape[0] // BLOCK
    lax.fori_loop(0, blocks // 2, block, 0)
    handed(64, 0)
    hand_on(tp, 0, 64, 2, ep, flips[3])
    hand_on(flips[1], 0, 64, 2, ep, flips[3])
    handed(64, 1)
    hand_on(tp, 64, 64, 3, ep, flips[1])
    hand_on(flips[3], 64, 64, 3, ep, flips[1])
    lax.fori_loop(blocks // 2, blocks, block, 0)
    msg[0:64, :] = sbd[0:64, 0:128]
    msg[64:128, :] = sbd[64:128, 128:256]
    msg[128:136, :] = total[...]
    first = remote(msg, pmsg, dd_ssem.at[0], dd_rsem.at[0], partner, tp)
    first.start()

    def column(row8):
        return jnp.exp(dot_t0(row8, jnp.ones((8, 128), F32), HIGH))

    def rows_of(j, p=None):
        lo, n = START[j] * CAP, SIZES[j] * CAP
        return slice(lo, lo + n) if p is None else slice(lo + p * n // 2, lo + (p + 1) * n // 2)

    def expert(j):
        n = SIZES[j]
        x_rows = recv2[START[j] : START[j] + n].reshape(n * CAP, recv2.shape[2])
        for lo in range(0, hid.shape[1], 256):
            cols = slice(lo, lo + 256)
            gate = dot(x_rows, wg[:, cols])
            up = dot(x_rows, wu[:, cols])
            hid[0 : n * CAP, cols] = (gate * jax.nn.sigmoid(gate) * up).astype(BF16)
        for m in (2, 1, 3, 0):
            cols = pl.ds(pl.multiple_of(flips[m] * 512, 512), 512)
            psend[m, rows_of(j), :] = dot(hid[0 : n * CAP, :], wdn[:, cols]).astype(BF16)
            for p, q, k in ((0, 1, 0), (0, 2, 1), (1, 3, 0), (1, 2, 1)):
                if q == m:
                    remote(
                        psend.at[m, rows_of(j, p)], r1.at[k, rows_of(j, p)],
                        rs_ssem, r1_rsem.at[j, p], ep, flips[1 + 2 * p],
                    ).start()

    def middle(j):
        for p in range(2):
            rows = rows_of(j, p)
            both = r1.at[:, rows]
            remote(both, both, rs_ssem, r1_rsem.at[j, p], ep, tp).wait_recv()
            pair = psend[3 - 2 * p, rows, :].astype(F32) + r1[1, rows, :].astype(F32)
            s2[rows, :] = pair.astype(BF16)
            remote(s2.at[rows], r2.at[rows], rs_ssem, r2_rsem.at[j, p], ep, flips[3 - 2 * p]).start()

    def reduce(j):
        for p in range(2):
            rows = rows_of(j, p)
            remote(r2.at[rows], r2.at[rows], rs_ssem, r2_rsem.at[j, p], ep, tp).wait_recv()
            whole = psend[0, rows, :].astype(F32) + r1[0, rows, :].astype(F32) + r2[rows, :].astype(F32)
            first_slot, n = START[j] + p * SIZES[j] // 2, SIZES[j] // 2
            rsend[first_slot : first_slot + n] = whole.astype(BF16).reshape(n, CAP, 512)
            for s in range(first_slot, first_slot + n):
                if s == 0:
                    rret[ep] = rsend[0]
                else:
                    to = target(ORDER[s], -1)
                    remote(rsend.at[s], rret.at[ep], rt_ssem, rt_rsem, to, tp).start()

    def arrived(j):
        for s in range(max(START[j], 1), START[j] + SIZES[j]):
            remote(recv2.at[s], recv2.at[s], dsend, drecv.at[s], ep, tp).wait_recv()

    first.wait_recv()
    later_core = c == 1
    mine, other = msg[0:128, :], pmsg[0:128, :]
    older = jnp.where(later_core, other, mine)
    newer = jnp.where(later_core, mine, other)
    newer_total = jnp.where(later_core, msg[128:136, :], pmsg[128:136, :])
    joint[...] = column(newer_total) * older + newer
    half = pl.ds(pl.multiple_of(c * 64, 64), 64)
    chmsg[0:64, :] = joint[half, :]
    chmsg[64:72, :] = msg[128:136, :] + pmsg[128:136, :]
    yrecv[y] = chmsg[...]

    def y_share(d):
        return remote(chmsg, yrecv.at[y], ch_ssem, y_rsem.at[d - 1], target((0, d, 0)), tp)

    def z_share(d):
        return remote(zmsg, zrecv.at[d - 1], zm_ssem.at[d - 1], z_rsem.at[d - 1], target((d, 0, 0)), tp)

    for d in range(1, NY):
        y_share(d).start()

    for d in NEAR:
        straight((d, 0, 1))
        straight((0, d, 1))
    leave(NEAR, NEAR)
    for i in range(7, 10):
        loads[i].wait()
    arrived(0)
    expert(0)
    pass_on(FAR, FAR)
    pass_on(FAR, NEAR)
    pass_on(NEAR, FAR)
    arrived(1)
    expert(1)
    middle(0)
    def fade_of(row8):
        fade = column(row8)
        return jnp.where(later_core, fade[64:128], fade[0:64])

    for d in range(1, NY):
        y_share(d).wait_recv()
    row_state, row_total = yrecv[0, 0:64, :], yrecv[0, 64:72, :]
    own_state = jnp.zeros_like(row_state)
    own_total = jnp.zeros_like(row_total)
    for k in range(1, NY):
        own_state = jnp.where(y == k, row_state, own_state)
        own_total = jnp.where(y == k, row_total, own_total)
        row_state = fade_of(yrecv[k, 64:72, :]) * row_state + yrecv[k, 0:64, :]
        row_total = row_total + yrecv[k, 64:72, :]
    ymsg[0:64, :], ymsg[64:72, :] = own_state, own_total
    zmsg[0:64, :], zmsg[64:72, :] = row_state, row_total
    for d in range(1, NZ):
        pl.when(z + d < NZ)(z_share(d).start)
    cols_in = jnp.concatenate(
        [routes_t_ref[...].astype(F32), share_t, jnp.zeros((4, rows2), F32)], axis=0
    )
    unit = (iota((8, 128), 0) == iota((8, 128), 1)).astype(F32)
    cols_out = dot_t0(cols_in, unit, HIGH)
    e_lane = iota((rows2, experts), 1).astype(F32)
    r_cols = [cols_out[:, 0:1], cols_out[:, 1:2]]
    member = ((r_cols[0] == e_lane) | (r_cols[1] == e_lane)).astype(BF16)
    earlier = (iota((rows2, rows2), 0) > iota((rows2, rows2), 1)).astype(BF16)
    rank = dot(earlier, member)
    lanes = iota((rows2, experts * CAP), 1).astype(F32)
    for r in range(2):
        slot = jnp.sum(jnp.where(r_cols[r] == e_lane, rank, 0.0), axis=1, keepdims=True)
        pickm[r] = (lanes == slot + r_cols[r] * CAP).astype(BF16)

    pass_on(NEAR, NEAR)
    reduce(0)
    middle(1)
    handed(128, 2)
    handed(128, 3)
    for m in range(1, 4):
        hand_on(flips[m], 0, 128, 4, partner, tp)
    arrived(2)
    expert(2)
    reduce(1)
    arrived(3)
    expert(3)
    inc[half, :] = jnp.zeros((64, 128), F32)

    def join(k, _):
        cp = remote(zrecv.at[z - k - 1], zrecv.at[z - k - 1], ch_ssem, z_rsem.at[z - k - 1], ep, tp)
        cp.wait_recv()
        fade = fade_of(zrecv[z - k - 1, 64:72, :])
        inc[half, :] = fade * inc[half, :] + zrecv[z - k - 1, 0:64, :]
        return 0

    lax.fori_loop(0, z, join, 0)
    inc[half, :] = fade_of(ymsg[64:72, :]) * inc[half, :] + ymsg[0:64, :]
    second = remote(inc.at[half], inc.at[half], dd_ssem.at[1], dd_rsem.at[1], partner, tp)
    second.start()
    middle(2)
    arrived(4)
    expert(4)
    second.wait()
    joined = column(pmsg[128:136, :]) * inc[...] + pmsg[0:128, :]
    entry = jnp.where(later_core, joined, inc[...])
    entry_bd = jnp.concatenate([entry, entry], axis=1) * own_head
    for i in range(att.shape[0] // 128):
        rows = slice(128 * i, 128 * i + 128)
        whole = att[rows, :] + dot(reach[rows, :], entry_bd, HIGH)
        parts = []
        for h in range(2):
            one = whole[:, VALUE_DIM * h : VALUE_DIM * (h + 1)]
            parts.append(one * lax.rsqrt(jnp.mean(one * one, axis=-1, keepdims=True) + EPS))
        out_gate = proj[rows, 512:768]
        rows_out = jnp.concatenate(parts, axis=1) * hgain_ref[...]
        gated[rows, :] = (rows_out * (out_gate * jax.nn.sigmoid(out_gate))).astype(BF16)
    quarter = out1_ref.shape[0]
    mine_cols = pl.ds(pl.multiple_of(tp * 256, 256), 256)
    spread[:, mine_cols] = gated[pl.ds(pl.multiple_of(tp * quarter, quarter), quarter), :]

    arrived(5)
    expert(5)
    middle(3)
    reduce(2)
    middle(4)
    middle(5)
    for m in range(1, 4):
        rows = pl.ds(pl.multiple_of(flips[m] * quarter, quarter), quarter)
        remote(gated.at[rows], spread.at[:, mine_cols], mx_ssem, mx_rsem, ep, flips[m]).start()
    reduce(3)
    reduce(4)
    reduce(5)
    remote(spread.at[:, 0:768], spread.at[:, 0:768], mx_ssem, mx_rsem, ep, tp).wait_recv()
    handed(384, 4)
    for n in range(4):
        cols = slice(512 * n, 512 * n + 512)
        out1_ref[:, cols] = dot(spread[...], wfull[:, cols]).astype(BF16)

    remote(rret.at[1:experts], rret.at[1:experts], rt_ssem, rt_rsem, ep, tp).wait_recv()
    flat = rret[...].reshape(experts * CAP, 512)
    mixed = jnp.zeros((rows2, 512), F32)
    for r in range(2):
        mixed = mixed + dot(pickm[r], flat) * cols_out[:, 2 + r : 3 + r]
    out2_ref[...] = mixed.astype(BF16)

    remote(send2.at[1:experts], send2.at[1:experts], dsend, drecv.at[0], ep, tp).wait_send()
    remote(relay, relay, dsend, drecv.at[0], ep, tp).wait_send()
    remote(r1, r1, rs_ssem, r1_rsem.at[0, 0], ep, tp).wait_send()
    remote(r2, r2, rs_ssem, r1_rsem.at[0, 0], ep, tp).wait_send()
    for n in (128, 256, 384):
        remote(wfull.at[0:n], wfull.at[0:n], w_ssem, w_rsem.at[0], ep, tp).wait_send()
    remote(spread.at[:, 0:768], spread.at[:, 0:768], mx_ssem, mx_rsem, ep, tp).wait_send()
    remote(rret.at[1:experts], rret.at[1:experts], rt_ssem, rt_rsem, ep, tp).wait_send()
    first.wait_send()
    remote(yrecv.at[0:3], yrecv.at[0:3], ch_ssem, y_rsem.at[0], ep, tp).wait_send()
    for d in range(1, NZ):
        pl.when(z + d < NZ)(z_share(d).wait_send)


def write_out(first_ref, second_ref, out1_ref, out2_ref):
    out1_ref[...] = first_ref[...]
    out2_ref[...] = second_ref[...]


def body(
    tokens_first, norm_gain_first, w_query, w_key, w_value, w_outgate, w_decay, decay_bias,
    head_gain, w_mix_out, tokens_second, norm_gain_second, routes, route_logits,
    expert_gate, expert_up, expert_down,
):
    hbm, vmem = pl.BlockSpec(memory_space=pl.ANY), pl.BlockSpec(memory_space=pltpu.VMEM)
    rows1, width = tokens_first.shape
    rows2 = tokens_second.shape[0]
    hidden = expert_gate.shape[2]
    experts = NZ * NY * NC
    quarter = width // 4
    V, D = pltpu.VMEM, pltpu.SemaphoreType.DMA
    first, second = pl.pallas_call(
        kernel,
        out_shape=(
            jax.ShapeDtypeStruct((rows1 // 4, width), BF16),
            jax.ShapeDtypeStruct((rows2, quarter), BF16),
        ),
        in_specs=[
            hbm, vmem, hbm, hbm, hbm, hbm, hbm, vmem, vmem, hbm,
            hbm, vmem, vmem, vmem, hbm, hbm, hbm,
        ],
        out_specs=(vmem, vmem),
        scratch_shapes=[
            V((rows2, width), BF16), V((rows2, width), BF16),
            V((experts, CAP, width), BF16), V((experts, CAP, width), BF16),
            V((18, CAP, width), BF16),
            V((rows1, width), BF16), V((rows1, width), BF16),
            V((width, 896), BF16), V((1024, width), BF16),
            V((width, hidden), BF16), V((width, hidden), BF16), V((hidden, width), BF16),
            V((rows1, 896), F32), V((rows1, 256), F32), V((rows1, 128), F32),
            V((128, 256), F32), V((8, 128), F32), V((136, 128), F32), V((136, 128), F32),
            V((128, 128), F32), V((128, 128), F32),
            V((4, experts * CAP, quarter), BF16), V((2, experts * CAP, quarter), BF16),
            V((experts * CAP, quarter), BF16), V((experts * CAP, quarter), BF16),
            V((experts, CAP, quarter), BF16), V((experts, CAP, quarter), BF16),
            V((rows1, 256), BF16), V((rows1 // 4, 1024), BF16),
            V((2, rows2, experts * CAP), BF16),
            V((max(SIZES) * CAP, hidden), BF16), V((72, 128), F32), V((72, 128), F32),
            V((72, 128), F32), V((NY, 72, 128), F32), V((NZ - 1, 72, 128), F32),
            D((11,)), D(()), D((32,)), D((18,)), D(()), D((CHUNKS, 2)), D((CHUNKS, 2)), D(()), D((5,)),
            D(()), D(()), D(()), D(()),
            D((2,)), D((2,)), D(()), D((3,)), D((3,)), D((3,)),
        ],
        compiler_params=pltpu.CompilerParams(
            collective_id=0, has_side_effects=True, vmem_limit_bytes=63 * 2**20
        ),
        name="layer",
    )(
        tokens_first, norm_gain_first.reshape(1, -1), w_query, w_key, w_value, w_outgate, w_decay,
        decay_bias, head_gain.reshape(1, -1), w_mix_out, tokens_second,
        norm_gain_second.reshape(1, -1), routes.T, route_logits.T,
        expert_gate, expert_up, expert_down,
    )
    return pl.pallas_call(
        write_out,
        out_shape=(
            jax.ShapeDtypeStruct(first.shape, BF16), jax.ShapeDtypeStruct(second.shape, BF16)
        ),
        in_specs=[vmem, vmem],
        out_specs=(vmem, vmem),
        compiler_params=pltpu.CompilerParams(vmem_limit_bytes=4 * 2**20),
        name="write_out",
    )(first, second)


def solution(mesh):
    ep_tp = ("ep", "tp")
    in_specs = (
        P("ep", None), P(), P(None, "tp"), P(None, "tp"), P(None, "tp"), P(None, "tp"),
        P(None, "tp"), P("ep", "tp"), P("tp"), P("tp", None), P("ep", None), P(), P("ep", None),
        P("ep", None), P("ep", None, "tp"), P("ep", None, "tp"), P("ep", "tp", None),
    )
    out_specs = (P(ep_tp, None), P("ep", "tp"))
    return jax.shard_map(body, mesh=mesh, in_specs=in_specs, out_specs=out_specs, check_vma=False)
```
